256 devices in a mesh: grp: 2 (over y), tp: 16 (over z), dp: 8 (over x, core).
Axes of the slice: x: 4, y: 2, z: 16, core: 2. Of those that a mesh axis runs over, the one named last changes fastest.
The devices are a block of a 4x16x16 slice.
Arguments:
- tokens: bfloat16 [512, 4096], P('grp', 'dp'), parts along dimension 0, may hold values from -40 to 40
- sequence_lengths: int32 [512], P(('grp', 'dp')), parts along dimension 0, may hold values from 1 to 4096, 262144 in all
- recurrent_state: float32 [2, 512, 128, 128], P(None, ('grp', 'dp'), 'tp'), parts along dimension 1, may hold values from -1.8 to 1.8
- norm_weight: float32 [2, 4096], P(None, 'dp'), may hold values from 0.1 to 1.9
- input_weight: bfloat16 [2, 4096, 2048], P(None, 'dp', 'tp'), may hold values from -0.09375 to 0.09375
- gate_weight: bfloat16 [2, 4096, 2048], P(None, 'dp', 'tp'), may hold values from -0.09375 to 0.09375
- output_weight: bfloat16 [2, 2048, 4096], P(None, 'tp', 'dp'), may hold values from -0.125 to 0.125
- negated_real_rate: float32 [2, 8192], P(None, 'tp'), may hold values from 0.005 to 1
- frequency: float32 [2, 8192], P(None, 'tp'), may hold values from -4 to 4
- discrete_step: float32 [2, 128], P(None, 'tp'), may hold values from 0.02 to 0.5
- group_input_matrix: float32 [2, 128, 16, 128], P(None, 'tp'), may hold values from -1.5 to 1.5
- group_output_matrix: float32 [2, 128, 16, 128], P(None, 'tp'), may hold values from -0.5 to 0.5
- feedthrough_weight: float32 [2, 2048], P(None, 'tp'), may hold values from -3 to 3
- extra_log_decay: float32 [2, 128, 4096], P(None, 'tp'), may hold values from -0.7 to 0
Outputs:
- tokens_out: bfloat16 [512, 4096], P('grp', 'dp'), parts along dimension 0
- state_out: float32 [2, 512, 128, 128], P(None, ('grp', 'dp'), 'tp'), parts along dimension 1
The draws below stay inside these ranges and needn't reach their ends.
There are 2 independent parts, one for each index of `grp`. The reference program is written for one: setup_inputs(seed, part) draws one part's arguments, and reference() takes and returns one part's arrays. A program takes and returns all parts, laid end to end along the dimension named above; an argument that names none is the same for every part. Nothing has to cross between parts.
Inputs may be any that keep to these rules, and one draw needn't show every extreme that they name: The newest token of a sequence stands at position sequence_lengths - 1.
All inputs are finite; a program needn't handle non-finite values. No bound on the sum of `sequence_lengths` on one device may be relied on, other than what follows from the above.
Results may differ from the reference program's by a relative error of at most 0.009.
Values may be sent and summed in bfloat16 or wider, within the bound.
A program may use at most 64 MiB of HBM per device.

```python
import math
import jax
import jax.numpy as jnp
import numpy as np
from jax import lax

D = 4096
N = 2048
GROUP = 16
P_SIZE = 64
CHANNEL_GROUPS = 128
STACKED_LAYERS = 2
BATCH = 256
LONGEST_LENGTH = 4096
MEAN_LEN = 1024


def draw_tokens(key, part):
    key_base = jax.random.fold_in(key, 11)
    key_rows = jax.random.fold_in(key, 12)
    key_cols = jax.random.fold_in(key, 13)
    base = jnp.clip(jax.random.normal(key_base, (BATCH, D), jnp.float32), -4.0, 4.0)
    rising = 4.0
    row_scale = jnp.exp(jax.random.uniform(key_rows, (BATCH, 1), jnp.float32, math.log(0.3), math.log(3.0)))
    column_pos = jnp.arange(D, dtype=jnp.float32)[None, :] / D
    jitter = jnp.exp(jax.random.uniform(key_cols, (1, D), jnp.float32, -0.5, 0.5))
    col_scale = 0.5 * jnp.exp(math.log(rising) * column_pos) * jitter
    return (base * row_scale * col_scale).astype(jnp.bfloat16)


def level_of(key, dims, pieces, least, largest):
    def one(position, blocks):
        heights = jax.random.uniform(jax.random.fold_in(jax.random.fold_in(key, 6), position), (blocks,), jnp.float32, least / len(pieces), largest / len(pieces))
        return jnp.repeat(jnp.exp(heights), dims[position] // blocks).reshape((-1,) + (1,) * (len(dims) - position - 1))

    loudness = one(*pieces[0])
    for cut in pieces[1:]:
        loudness = loudness * one(*cut)
    return loudness


def profile(amount, total, most, slope):
    weights = [(1 << 20) // math.isqrt(grade ** slope) + 1 for grade in range(2, amount + 1)]
    rest, counts = total - most - (amount - 1), [1] * (amount - 1)
    while rest > 0:
        free = [i for i in range(amount - 1) if counts[i] < most]
        mass, left = sum([weights[i] for i in free]), rest
        for i in free:
            addition = min(most - counts[i], max(1, left * weights[i] // mass), rest)
            counts[i] = counts[i] + addition
            rest = rest - addition
    return np.array([most] + counts)


def uneven_parts(stream_key, amount, total, bound, skew):
    if amount == 2:
        one = jax.random.randint(stream_key, (), max(1, total - bound), min(bound, total - 1) + 1)
        return jnp.stack([one, total - one])
    lengths = jnp.asarray(profile(amount, total, bound, skew), jnp.int32)
    couples = (amount - 1) // 2
    source_of, receiver = lengths[1:1 + 2 * couples:2], lengths[2:2 + 2 * couples:2]
    margin = jnp.minimum(source_of - 1, bound - receiver)
    passed = jax.random.randint(jax.random.fold_in(stream_key, 1), (couples,), 0, 1 << 20) % (margin + 1)
    lengths = lengths.at[1:1 + 2 * couples:2].set(source_of - passed).at[2:2 + 2 * couples:2].set(receiver + passed)
    return lengths[jax.random.permutation(jax.random.fold_in(stream_key, 2), amount)]


def centred(key, dims, scale, limit, split=(), kind=jnp.bfloat16):
    gain = level_of(key, dims, split, -0.22, 0.18) if split else 1.0
    values = jax.random.normal(key, dims, jnp.float32) * scale * gain
    return jnp.minimum(jnp.maximum(values, -limit), limit).astype(kind)


def setup_inputs(seed: int = 0, part: int = 0) -> dict:
    arg_keys = jax.random.split(jax.random.key(seed), 15)
    own_keys = jax.random.split(jax.random.fold_in(arg_keys[14], part), 15)
    tokens = draw_tokens(jax.random.fold_in(jax.random.fold_in(arg_keys[14], part), 71), part)
    sequence_lengths = uneven_parts(own_keys[1], BATCH, BATCH * MEAN_LEN, LONGEST_LENGTH, 2).astype(jnp.int32)
    recurrent_state = centred(own_keys[2], (STACKED_LAYERS, BATCH, CHANNEL_GROUPS, 2 * P_SIZE), 0.3, 1.8, ((1, 8), (2, 16)), jnp.float32)
    norm_weight = jnp.clip(1.0 + 0.18 * jax.random.normal(arg_keys[3], (STACKED_LAYERS, D), jnp.float32), 0.1, 1.9)
    input_weight = centred(arg_keys[4], (STACKED_LAYERS, D, N), D ** -0.5, 0.09375, ((1, 8), (2, 16)))
    gate_weight = centred(arg_keys[5], (STACKED_LAYERS, D, N), D ** -0.5, 0.09375, ((1, 8), (2, 16)))
    output_weight = centred(arg_keys[6], (STACKED_LAYERS, N, D), N ** -0.5, 0.125, ((1, 16), (2, 8)))
    negated_real_rate = jnp.clip(jnp.exp(math.log(1.0) - 5.2983174 * jax.random.uniform(arg_keys[7], (STACKED_LAYERS, CHANNEL_GROUPS * P_SIZE), jnp.float32) ** level_of(arg_keys[7], (STACKED_LAYERS, CHANNEL_GROUPS * P_SIZE), ((1, 16),), -0.2, 0.2)), 0.005, 1.0)
    frequency = jnp.clip(jax.random.uniform(arg_keys[8], (STACKED_LAYERS, CHANNEL_GROUPS * P_SIZE), jnp.float32, -4.0, 4.0) * level_of(arg_keys[8], (STACKED_LAYERS, CHANNEL_GROUPS * P_SIZE), ((1, 16),), -0.4, 0.0), -4.0, 4.0)
    discrete_step = jnp.clip(jnp.exp(math.log(0.5) - 3.218876 * jax.random.uniform(arg_keys[9], (STACKED_LAYERS, CHANNEL_GROUPS), jnp.float32) ** level_of(arg_keys[9], (STACKED_LAYERS, CHANNEL_GROUPS), ((1, 16),), -0.2, 0.2)), 0.02, 0.5)
    group_input_matrix = centred(arg_keys[10], (STACKED_LAYERS, CHANNEL_GROUPS, GROUP, 2 * P_SIZE), GROUP ** -0.5, 1.5, ((1, 16),), jnp.float32)
    group_output_matrix = centred(arg_keys[11], (STACKED_LAYERS, CHANNEL_GROUPS, GROUP, 2 * P_SIZE), (2 * P_SIZE) ** -0.5, 0.5, ((1, 16),), jnp.float32)
    feedthrough_weight = centred(arg_keys[12], (STACKED_LAYERS, N), 0.5, 3.0, ((1, 16),), jnp.float32)
    extra_log_decay = jnp.clip(-0.7 + 0.7 * jax.random.uniform(arg_keys[13], (STACKED_LAYERS, CHANNEL_GROUPS, LONGEST_LENGTH), jnp.float32) ** level_of(arg_keys[13], (STACKED_LAYERS, CHANNEL_GROUPS, LONGEST_LENGTH), ((1, 16),), -0.2, 0.2), -0.7, 0.0)
    return dict(tokens=tokens, sequence_lengths=sequence_lengths, recurrent_state=recurrent_state, norm_weight=norm_weight, input_weight=input_weight, gate_weight=gate_weight, output_weight=output_weight, negated_real_rate=negated_real_rate, frequency=frequency, discrete_step=discrete_step, group_input_matrix=group_input_matrix, group_output_matrix=group_output_matrix, feedthrough_weight=feedthrough_weight, extra_log_decay=extra_log_decay)


TOP_PRECISION = lax.Precision.HIGHEST
NORM_EPS = 1e-06

def transition(decay_factor, angular_frequency, step_width):
    log_mag = -decay_factor * step_width[:, None]
    turn = angular_frequency * step_width[:, None]
    magnitude = jnp.exp(log_mag)
    discrete_real = magnitude * jnp.cos(turn)
    discrete_imaginary = magnitude * jnp.sin(turn)
    half_sine = jnp.sin(0.5 * turn)
    numer_re = jnp.expm1(log_mag) * jnp.cos(turn) - 2.0 * half_sine * half_sine
    numer_im = discrete_imaginary
    denom = decay_factor * decay_factor + angular_frequency * angular_frequency
    drive_re = (-numer_re * decay_factor + numer_im * angular_frequency) / denom
    drive_im = (-numer_im * decay_factor - numer_re * angular_frequency) / denom
    return (discrete_real, discrete_imaginary, drive_re, drive_im)

def state_space_update(input_groups, layer_state, extra_decay_factor, decay_factor, angular_frequency, step_width, input_matrix, readout_matrix):
    half_width = input_matrix.shape[-1] // 2
    decay_factor = decay_factor.reshape(-1, half_width)
    angular_frequency = angular_frequency.reshape(-1, half_width)
    discrete_real, discrete_imaginary, drive_re, drive_im = transition(decay_factor, angular_frequency, step_width)
    input_real = input_matrix[..., :half_width]
    input_imaginary = input_matrix[..., half_width:]
    driven_input_real = jnp.einsum('tkl,klf->tkf', input_groups, input_real, precision=TOP_PRECISION)
    driven_input_imaginary = jnp.einsum('tkl,klf->tkf', input_groups, input_imaginary, precision=TOP_PRECISION)
    state_re = layer_state[..., :half_width]
    state_im = layer_state[..., half_width:]
    carried_real = extra_decay_factor[..., None] * discrete_real[None]
    carried_imaginary = extra_decay_factor[..., None] * discrete_imaginary[None]
    updated_real = carried_real * state_re - carried_imaginary * state_im + drive_re[None] * driven_input_real - drive_im[None] * driven_input_imaginary
    updated_imaginary = carried_real * state_im + carried_imaginary * state_re + drive_re[None] * driven_input_imaginary + drive_im[None] * driven_input_real
    readout_rows = jnp.einsum('hzk,dhk->dhz', readout_matrix[..., :half_width], updated_real, precision=TOP_PRECISION) - jnp.einsum('hzk,dhk->dhz', readout_matrix[..., half_width:], updated_imaginary, precision=TOP_PRECISION)
    return (readout_rows, jnp.concatenate([updated_real, updated_imaginary], axis=-1))

def single_layer(hidden_rows, sequence_lengths, layer_state, norm_scale_rows, input_matrix_weight, gate_matrix, output_matrix_weight, decay_factor, angular_frequency, step_width, input_matrix, readout_matrix, feedthrough_rows, extra_decay_rows):
    x_float = hidden_rows.astype(jnp.float32)
    scale = lax.rsqrt(lax.optimization_barrier(jnp.mean(x_float * x_float, axis=1)) + NORM_EPS)[:, None]
    scaled_in = (x_float * norm_scale_rows[None, :]).astype(jnp.bfloat16)
    u_vals = (jnp.dot(scaled_in, input_matrix_weight, preferred_element_type=jnp.float32) * scale).astype(jnp.bfloat16)
    gate_vals = (jnp.dot(scaled_in, gate_matrix, preferred_element_type=jnp.float32) * scale).astype(jnp.bfloat16)
    batch_rows = hidden_rows.shape[0]
    group_count = layer_state.shape[1]
    input_float = u_vals.astype(jnp.float32)
    token_positions = (sequence_lengths - 1).astype(jnp.int32)
    extra_decay_factor = jnp.exp(jnp.take(extra_decay_rows, token_positions, axis=1).T)
    readout_rows, updated_state = state_space_update(input_float.reshape(batch_rows, group_count, -1), layer_state, extra_decay_factor, decay_factor, angular_frequency, step_width, input_matrix, readout_matrix)
    y_vals = jax.nn.gelu(readout_rows.reshape(batch_rows, -1) + feedthrough_rows[None, :] * input_float)
    mixed = (y_vals * jax.nn.sigmoid(gate_vals.astype(jnp.float32))).astype(jnp.bfloat16)
    branch = jnp.dot(mixed, output_matrix_weight, preferred_element_type=jnp.float32).astype(jnp.bfloat16)
    x_next = (x_float + branch.astype(jnp.float32)).astype(jnp.bfloat16)
    return (x_next, updated_state)

def reference(tokens, sequence_lengths, recurrent_state, norm_weight, input_weight, gate_weight, output_weight, negated_real_rate, frequency, discrete_step, group_input_matrix, group_output_matrix, feedthrough_weight, extra_log_decay):
    hidden_rows = tokens
    states = []
    for index_of_layer in range(STACKED_LAYERS):
        hidden_rows, updated_state = single_layer(hidden_rows, sequence_lengths, recurrent_state[index_of_layer], norm_weight[index_of_layer], input_weight[index_of_layer], gate_weight[index_of_layer], output_weight[index_of_layer], negated_real_rate[index_of_layer], frequency[index_of_layer], discrete_step[index_of_layer], group_input_matrix[index_of_layer], group_output_matrix[index_of_layer], feedthrough_weight[index_of_layer], extra_log_decay[index_of_layer])
        states.append(updated_state)
    return (hidden_rows, jnp.stack(states, axis=0))
```

```python
import functools

import jax
import jax.numpy as jnp
from jax import lax
from jax.experimental import pallas as pl
from jax.experimental.pallas import tpu as pltpu
from jax.sharding import PartitionSpec as P

NORM_EPS = 1e-06
HIGHEST = lax.Precision.HIGHEST
F32 = jnp.float32
BF16 = jnp.bfloat16
MESH = pl.DeviceIdType.MESH


def contract_last(a, b, precision=None):
    return lax.dot_general(
        a, b, (((1,), (1,)), ((), ())), precision=precision, preferred_element_type=F32
    )


def split_two(a):
    high = a.astype(BF16)
    return high, (a - high.astype(F32)).astype(BF16)


def exp_less_one(x, exp_x):
    series = jnp.full_like(x, 1.0 / 3628800.0)
    for factor in (362880.0, 40320.0, 5040.0, 720.0, 120.0, 24.0, 6.0, 2.0, 1.0):
        series = series * x + 1.0 / factor
    return jnp.where(jnp.abs(x) < 0.6, series * x, exp_x - 1.0)


def kernel(
    n_dp,
    n_tp,
    features,
    lengths,
    step_width,
    tokens_hbm,
    norm_hbm,
    w_in_hbm,
    w_gate_hbm,
    decay_hbm,
    state_hbm,
    rate_hbm,
    freq_hbm,
    b_hbm,
    c_hbm,
    feed_hbm,
    w_out_hbm,
    tokens_out,
    state_out,
    x_buf,
    norm,
    w_cat,
    w_out,
    decay,
    state,
    rate,
    freq,
    b_mat,
    c_mat,
    feed,
    local_sem,
    out_sem,
    part_buf,
    part_recv,
    part_send_sem,
    part_recv_sem,
    sq_buf,
    sq_recv,
    sq_send_sem,
    sq_recv_sem,
    z_buf,
    z_send_sem,
    z_recv_sem,
    term_buf,
    term_recv,
    term_send_sem,
    term_recv_sem,
    x_send_sem,
    x_recv_sem,
    pick,
    carried,
    drive_high,
    drive_low,
    mix_cat,
    base,
):
    i = lax.axis_index("dp")
    j = lax.axis_index("tp")
    layers, mine, groups, width = state.shape
    half = width // 2
    rows, local_d = x_buf.shape[1:]
    chans = w_out.shape[1]
    chunk = rows // n_tp
    per_block = mine // chunk
    channel_group = chans // groups

    dp_steps = [(0, 1)] + [
        (d, e) for d in (1, n_dp // 2 - 1, 2) for e in (0, 1)
    ]

    def dp_peer(step):
        d, e = step
        return lax.rem(lax.div(i, 2) + d, n_dp // 2) * 2 + lax.rem(lax.rem(i, 2) + e, 2)

    tp_steps = []
    for d in range(1, n_tp // 2 + 1):
        tp_steps.append(d)
        if n_tp - d != d:
            tp_steps.append(n_tp - d)

    def tp_peer(step):
        return lax.rem(j + step, n_tp)

    barrier = pltpu.get_barrier_semaphore()
    for step in dp_steps:
        pl.semaphore_signal(barrier, inc=1, device_id={"dp": dp_peer(step)}, device_id_type=MESH)
    for step in tp_steps:
        pl.semaphore_signal(barrier, inc=1, device_id={"tp": tp_peer(step)}, device_id_type=MESH)

    loads = {}
    for n, (name, src, dst) in enumerate(
        [
            ("x", tokens_hbm, x_buf.at[0]),
            ("norm", norm_hbm, norm),
            ("w_in", w_in_hbm, w_cat.at[:, :, pl.ds(0, chans)]),
            ("w_gate", w_gate_hbm, w_cat.at[:, :, pl.ds(chans, chans)]),
            ("decay", decay_hbm, decay),
            ("state", state_hbm, state),
            ("rate", rate_hbm, rate),
            ("freq", freq_hbm, freq),
            ("b", b_hbm, b_mat),
            ("c", c_hbm, c_mat),
            ("feed", feed_hbm, feed),
            ("w_out", w_out_hbm, w_out),
        ]
    ):
        loads[name] = pltpu.make_async_copy(src, dst, local_sem.at[n])
        loads[name].start()

    lane = lax.broadcasted_iota(jnp.int32, (groups, width), 1)
    sub = lax.broadcasted_iota(jnp.int32, (groups, width), 0)
    low = lane < half
    col_group = lax.broadcasted_iota(jnp.int32, (groups, chans), 1) // channel_group
    own_group = col_group == lax.broadcasted_iota(jnp.int32, (groups, chans), 0)
    block_row = lax.broadcasted_iota(jnp.int32, (chans, chans), 0) // channel_group
    block_col = lax.broadcasted_iota(jnp.int32, (chans, chans), 1) // channel_group

    def by_group(ref, layer):
        out = jnp.zeros((groups, width), F32)
        for g in range(groups):
            pair = ref[layer : layer + 1, (g // 2) * width : (g // 2 + 1) * width]
            other = pltpu.roll(pair, half, 1)
            row = jnp.where(low[:1] if g % 2 == 0 else ~low[:1], pair, other)
            out = jnp.where(sub == g, row, out)
        return out

    def prepare(layer):
        dt = jnp.zeros((groups, width), F32)
        for g in range(groups):
            dt = jnp.where(sub == g, step_width[layer, g], dt)
        a_re = by_group(rate, layer)
        a_im = by_group(freq, layer)
        log_mag = -a_re * dt
        turn = a_im * dt
        magnitude = jnp.exp(log_mag)
        cosine = jnp.cos(turn)
        disc_re = magnitude * cosine
        disc_im = magnitude * jnp.sin(turn)
        half_sine = jnp.sin(0.5 * turn)
        numer_re = exp_less_one(log_mag, magnitude) * cosine - 2.0 * half_sine * half_sine
        denom = a_re * a_re + a_im * a_im
        drive_re = (-numer_re * a_re + disc_im * a_im) / denom
        drive_im = (-disc_im * a_re - numer_re * a_im) / denom
        disc_cross = jnp.where(low, -disc_im, disc_im)
        drive_cross = jnp.where(low, -drive_im, drive_im)

        b_l = b_mat[layer]
        drive = drive_re[:, None, :] * b_l + drive_cross[:, None, :] * pltpu.roll(b_l, half, 2)
        drive = drive.reshape(chans, width)
        high, rest = split_two(drive)
        drive_high[layer] = high
        drive_low[layer] = rest
        c_l = jnp.where(low[:1][None], c_mat[layer], -c_mat[layer]).reshape(chans, width)
        mix = jnp.where(block_row == block_col, contract_last(drive, c_l, HIGHEST), 0.0)
        high, rest = split_two(mix)
        mix_cat[layer, :chans] = high
        mix_cat[layer, chans:] = rest

        for r in range(mine):
            offset = lane - (lengths[r] - 1)
            found = jnp.zeros((groups, width), F32)
            for at in range(0, decay.shape[2], width):
                found = jnp.where(offset == -at, decay[layer, :, at : at + width], found)
            pick[r] = found
        extra = jnp.exp(jnp.sum(pick[...], axis=-1, keepdims=True))
        s = state[layer]
        kept = extra * (disc_re[None] * s + disc_cross[None] * pltpu.roll(s, half, 2))
        carried[layer] = kept
        read = contract_last(kept.reshape(mine * groups, width), c_l, HIGHEST)
        read = jnp.where(own_group[None], read.reshape(mine, groups, chans), 0.0)
        base[layer] = jnp.sum(read, axis=1)

    def send_part(layer, s):
        for src, dst, ssem, rsem in (
            (part_buf, part_recv, part_send_sem, part_recv_sem),
            (sq_buf, sq_recv, sq_send_sem, sq_recv_sem),
        ):
            pltpu.make_async_remote_copy(
                src_ref=src.at[layer, s],
                dst_ref=dst.at[layer, i],
                send_sem=ssem.at[layer, s],
                recv_sem=rsem.at[layer, i],
                device_id={"dp": s},
                device_id_type=MESH,
            ).start()

    ones = jnp.ones((8, 128), F32)

    def square_rows(x):
        x2 = x * x
        total = x2[:, 0:128]
        for k in range(1, local_d // 128):
            total = total + x2[:, k * 128 : (k + 1) * 128]
        return contract_last(ones, total, HIGHEST)

    sends = []

    loads["x"].wait()
    loads["norm"].wait()
    x = x_buf[0].astype(F32)
    scaled = (x * norm[0:1, :]).astype(BF16)
    squares = square_rows(x)
    for s in range(n_dp):
        sq_buf[0, s, :, pl.ds(0, mine)] = squares[:, s * mine : (s + 1) * mine]
    loads["w_in"].wait()
    loads["w_gate"].wait()
    part_buf[0] = (
        jnp.dot(scaled, w_cat[0], preferred_element_type=F32)
        .astype(BF16)
        .reshape(n_dp, mine, 2 * chans)
    )
    for name in ("decay", "state", "rate", "freq", "b", "c", "feed", "w_out"):
        loads[name].wait()
    pl.semaphore_wait(barrier, len(dp_steps) + len(tp_steps))
    for step in dp_steps:
        send_part(0, dp_peer(step))
    for layer in range(layers):
        prepare(layer)

    row_lane = lax.broadcasted_iota(jnp.int32, (mine, 128), 1)
    row_sub = lax.broadcasted_iota(jnp.int32, (mine, 128), 0)

    for layer in range(layers):
        total = part_buf[layer, i].astype(F32)
        sq = sq_buf[layer, i]
        for step in dp_steps:
            s = dp_peer(step)
            for src, dst, ssem, rsem in (
                (part_buf, part_recv, part_send_sem, part_recv_sem),
                (sq_buf, sq_recv, sq_send_sem, sq_recv_sem),
            ):
                pltpu.make_async_remote_copy(
                    src_ref=src.at[layer, s],
                    dst_ref=dst.at[layer, s],
                    send_sem=ssem.at[layer, s],
                    recv_sem=rsem.at[layer, s],
                    device_id={"dp": s},
                    device_id_type=MESH,
                ).wait_recv()
            total = total + part_recv[layer, s].astype(F32)
            sq = sq + sq_recv[layer, s]
        mean = jnp.sum(
            jnp.where(row_lane == row_sub, sq[0:1, :], 0.0), axis=1, keepdims=True
        ) / features
        scale = lax.rsqrt(mean + NORM_EPS)
        total = total * scale
        u = total[:, :chans].astype(BF16)
        gate = total[:, chans:].astype(BF16).astype(F32)
        u_f = u.astype(F32)
        read = base[layer] + jnp.dot(
            jnp.concatenate([u, u], axis=1), mix_cat[layer], preferred_element_type=F32
        )
        y = jax.nn.gelu(read + feed[layer : layer + 1, :] * u_f)
        z_buf[layer, i] = (y * jax.nn.sigmoid(gate)).astype(BF16)
        for step in dp_steps:
            s = dp_peer(step)
            pltpu.make_async_remote_copy(
                src_ref=z_buf.at[layer, i],
                dst_ref=z_buf.at[layer, i],
                send_sem=z_send_sem.at[layer, s],
                recv_sem=z_recv_sem.at[layer, i],
                device_id={"dp": s},
                device_id_type=MESH,
            ).start()

        for step in [(0, 0)] + dp_steps:
            s = dp_peer(step)
            if step != (0, 0):
                pltpu.make_async_remote_copy(
                    src_ref=z_buf.at[layer, s],
                    dst_ref=z_buf.at[layer, s],
                    send_sem=z_send_sem.at[layer, s],
                    recv_sem=z_recv_sem.at[layer, s],
                    device_id={"dp": s},
                    device_id_type=MESH,
                ).wait_recv()
            terms = jnp.dot(z_buf[layer, s], w_out[layer], preferred_element_type=F32)
            for k in range(per_block):
                t = s * per_block + k
                term_buf[layer, t] = terms[k * chunk : (k + 1) * chunk].astype(BF16)

                @pl.when(t != j)
                def _():
                    pltpu.make_async_remote_copy(
                        src_ref=term_buf.at[layer, t],
                        dst_ref=term_recv.at[layer, j],
                        send_sem=term_send_sem.at[layer, t],
                        recv_sem=term_recv_sem.at[layer, j],
                        device_id={"tp": t},
                        device_id_type=MESH,
                    ).start()

        spread = jnp.where(own_group[None], u_f[:, None, :], 0.0).astype(BF16)
        spread = spread.reshape(mine * groups, chans)
        driven = jnp.dot(spread, drive_high[layer], preferred_element_type=F32) + jnp.dot(
            spread, drive_low[layer], preferred_element_type=F32
        )
        carried[layer] = carried[layer] + driven.reshape(mine, groups, width)
        pltpu.make_async_copy(carried.at[layer], state_out.at[layer], out_sem.at[layer]).start()

        total = term_buf[layer, j].astype(F32)
        for step in tp_steps:
            t = tp_peer(step)
            pltpu.make_async_remote_copy(
                src_ref=term_buf.at[layer, t],
                dst_ref=term_recv.at[layer, t],
                send_sem=term_send_sem.at[layer, t],
                recv_sem=term_recv_sem.at[layer, t],
                device_id={"tp": t},
                device_id_type=MESH,
            ).wait_recv()
            total = total + term_recv[layer, t].astype(F32)
        at = pl.ds(pl.multiple_of(j * chunk, chunk), chunk)
        branch = total.astype(BF16).astype(F32)
        x_buf[layer + 1, at, :] = (x_buf[layer, at, :].astype(F32) + branch).astype(BF16)
        for step in tp_steps:
            t = tp_peer(step)
            pltpu.make_async_remote_copy(
                src_ref=x_buf.at[layer + 1, at],
                dst_ref=x_buf.at[layer + 1, at],
                send_sem=x_send_sem.at[layer, t],
                recv_sem=x_recv_sem.at[layer, j],
                device_id={"tp": t},
                device_id_type=MESH,
            ).start()

        def await_chunk(t):
            piece = pl.ds(pl.multiple_of(t * chunk, chunk), chunk)
            pltpu.make_async_remote_copy(
                src_ref=x_buf.at[layer + 1, piece],
                dst_ref=x_buf.at[layer + 1, piece],
                send_sem=x_send_sem.at[layer, t],
                recv_sem=x_recv_sem.at[layer, t],
                device_id={"tp": t},
                device_id_type=MESH,
            ).wait_recv()

        if layer + 1 < layers:
            order = [0]
            for d in range(1, n_dp // 2 + 1):
                order.append(d)
                if n_dp - d != d:
                    order.append(n_dp - d)
            for d in order:
                s = lax.rem(lax.div(j, per_block) + d, n_dp)
                for k in range(per_block):
                    t = s * per_block + k
                    if d == 0:
                        pl.when(t != j)(functools.partial(await_chunk, t))
                    else:
                        await_chunk(t)
                piece = pl.ds(pl.multiple_of(s * mine, mine), mine)
                x = x_buf[layer + 1, piece, :].astype(F32)
                scaled = (x * norm[layer + 1 : layer + 2, :]).astype(BF16)
                sq_buf[layer + 1, s, :, pl.ds(0, mine)] = square_rows(x)
                part_buf[layer + 1, s] = jnp.dot(
                    scaled, w_cat[layer + 1], preferred_element_type=F32
                ).astype(BF16)
                pl.when(s != i)(functools.partial(send_part, layer + 1, s))
        else:
            for step in tp_steps:
                await_chunk(tp_peer(step))
            pltpu.make_async_copy(x_buf.at[layers], tokens_out, out_sem.at[layers]).start()

    for layer in range(layers):
        for step in dp_steps:
            s = dp_peer(step)
            for src, dst, ssem, rsem in (
                (part_buf, part_recv, part_send_sem, part_recv_sem),
                (sq_buf, sq_recv, sq_send_sem, sq_recv_sem),
            ):
                pltpu.make_async_remote_copy(
                    src_ref=src.at[layer, s],
                    dst_ref=dst.at[layer, i],
                    send_sem=ssem.at[layer, s],
                    recv_sem=rsem.at[layer, i],
                    device_id={"dp": s},
                    device_id_type=MESH,
                ).wait_send()
            pltpu.make_async_remote_copy(
                src_ref=z_buf.at[layer, i],
                dst_ref=z_buf.at[layer, i],
                send_sem=z_send_sem.at[layer, s],
                recv_sem=z_recv_sem.at[layer, i],
                device_id={"dp": s},
                device_id_type=MESH,
            ).wait_send()
        for step in tp_steps:
            t = tp_peer(step)
            pltpu.make_async_remote_copy(
                src_ref=term_buf.at[layer, t],
                dst_ref=term_recv.at[layer, j],
                send_sem=term_send_sem.at[layer, t],
                recv_sem=term_recv_sem.at[layer, j],
                device_id={"tp": t},
                device_id_type=MESH,
            ).wait_send()
            at = pl.ds(pl.multiple_of(j * chunk, chunk), chunk)
            pltpu.make_async_remote_copy(
                src_ref=x_buf.at[layer + 1, at],
                dst_ref=x_buf.at[layer + 1, at],
                send_sem=x_send_sem.at[layer, t],
                recv_sem=x_recv_sem.at[layer, j],
                device_id={"tp": t},
                device_id_type=MESH,
            ).wait_send()
        pltpu.make_async_copy(carried.at[layer], state_out.at[layer], out_sem.at[layer]).wait()
    pltpu.make_async_copy(x_buf.at[layers], tokens_out, out_sem.at[layers]).wait()


def on_device(
    n_dp,
    n_tp,
    tokens,
    sequence_lengths,
    recurrent_state,
    norm_weight,
    input_weight,
    gate_weight,
    output_weight,
    negated_real_rate,
    frequency,
    discrete_step,
    group_input_matrix,
    group_output_matrix,
    feedthrough_weight,
    extra_log_decay,
):
    layers, mine, groups, width = recurrent_state.shape
    rows, local_d = tokens.shape
    chans = output_weight.shape[1]
    chunk = rows // n_tp
    smem = pl.BlockSpec(memory_space=pltpu.SMEM)
    hbm = pl.BlockSpec(memory_space=pl.ANY)
    dma = pltpu.SemaphoreType.DMA
    like = lambda a: pltpu.VMEM(a.shape, a.dtype)
    scratch = [
        pltpu.VMEM((layers + 1, rows, local_d), BF16),
        like(norm_weight),
        pltpu.VMEM((layers, local_d, 2 * chans), BF16),
        like(output_weight),
        like(extra_log_decay),
        like(recurrent_state),
        like(negated_real_rate),
        like(frequency),
        like(group_input_matrix),
        like(group_output_matrix),
        like(feedthrough_weight),
        dma((12,)),
        dma((layers + 1,)),
        pltpu.VMEM((layers, n_dp, mine, 2 * chans), BF16),
        pltpu.VMEM((layers, n_dp, mine, 2 * chans), BF16),
        dma((layers, n_dp)),
        dma((layers, n_dp)),
        pltpu.VMEM((layers, n_dp, 8, 128), F32),
        pltpu.VMEM((layers, n_dp, 8, 128), F32),
        dma((layers, n_dp)),
        dma((layers, n_dp)),
        pltpu.VMEM((layers, n_dp, mine, chans), BF16),
        dma((layers, n_dp)),
        dma((layers, n_dp)),
        pltpu.VMEM((layers, n_tp, chunk, local_d), BF16),
        pltpu.VMEM((layers, n_tp, chunk, local_d), BF16),
        dma((layers, n_tp)),
        dma((layers, n_tp)),
        dma((layers, n_tp)),
        dma((layers, n_tp)),
        pltpu.VMEM((mine, groups, width), F32),
        pltpu.VMEM((layers, mine, groups, width), F32),
        pltpu.VMEM((layers, chans, width), BF16),
        pltpu.VMEM((layers, chans, width), BF16),
        pltpu.VMEM((layers, 2 * chans, chans), BF16),
        pltpu.VMEM((layers, mine, chans), F32),
    ]
    return pl.pallas_call(
        functools.partial(kernel, n_dp, n_tp, n_dp * local_d),
        out_shape=(
            jax.ShapeDtypeStruct(tokens.shape, tokens.dtype),
            jax.ShapeDtypeStruct(recurrent_state.shape, recurrent_state.dtype),
        ),
        in_specs=[smem, smem] + [hbm] * 12,
        out_specs=(hbm, hbm),
        scratch_shapes=scratch,
        compiler_params=pltpu.CompilerParams(collective_id=0, has_side_effects=True),
    )(
        sequence_lengths,
        discrete_step,
        tokens,
        norm_weight,
        input_weight,
        gate_weight,
        extra_log_decay,
        recurrent_state,
        negated_real_rate,
        frequency,
        group_input_matrix,
        group_output_matrix,
        feedthrough_weight,
        output_weight,
    )


def solution(mesh):
    in_specs = (
        P("grp", "dp"),
        P(("grp", "dp")),
        P(None, ("grp", "dp"), "tp", None),
        P(None, "dp"),
        P(None, "dp", "tp"),
        P(None, "dp", "tp"),
        P(None, "tp", "dp"),
        P(None, "tp"),
        P(None, "tp"),
        P(None, "tp"),
        P(None, "tp", None, None),
        P(None, "tp", None, None),
        P(None, "tp"),
        P(None, "tp", None),
    )
    out_specs = (P("grp", "dp"), P(None, ("grp", "dp"), "tp", None))
    return jax.shard_map(
        functools.partial(on_device, mesh.shape["dp"], mesh.shape["tp"]),
        mesh=mesh,
        in_specs=in_specs,
        out_specs=out_specs,
        check_vma=False,
    )
```

```python
import functools

import jax
import jax.numpy as jnp
from jax import lax
from jax.experimental import pallas as pl
from jax.experimental.pallas import tpu as pltpu
from jax.sharding import PartitionSpec as P

NORM_EPS = 1e-06
HIGHEST = lax.Precision.HIGHEST
F32 = jnp.float32
BF16 = jnp.bfloat16
MESH = pl.DeviceIdType.MESH


def contract_last(a, b, precision=None):
    return lax.dot_general(
        a, b, (((1,), (1,)), ((), ())), precision=precision, preferred_element_type=F32
    )


def split_two(a):
    high = a.astype(BF16)
    return high, (a - high.astype(F32)).astype(BF16)


def exp_less_one(x, exp_x):
    series = jnp.full_like(x, 1.0 / 3628800.0)
    for factor in (362880.0, 40320.0, 5040.0, 720.0, 120.0, 24.0, 6.0, 2.0, 1.0):
        series = series * x + 1.0 / factor
    return jnp.where(jnp.abs(x) < 0.6, series * x, exp_x - 1.0)


def sign(o):
    return 1 if o > 0 else -1


def step_to_hub(o):
    near = (abs(o) + 1) // 3 * 3
    return abs(o) if near in (0, abs(o)) else abs(o) - near


def kernel(
    n_dp,
    n_tp,
    features,
    lengths,
    step_width,
    tokens_hbm,
    norm_hbm,
    w_in_hbm,
    w_gate_hbm,
    decay_hbm,
    state_hbm,
    rate_hbm,
    freq_hbm,
    b_hbm,
    c_hbm,
    feed_hbm,
    w_out_hbm,
    tokens_out,
    state_out,
    x_buf,
    norm,
    w_cat,
    w_out,
    decay,
    state,
    rate,
    freq,
    b_mat,
    c_mat,
    feed,
    local_sem,
    out_sem,
    part_buf,
    part_recv,
    part_send_sem,
    part_recv_sem,
    sq_buf,
    sq_recv,
    sq_send_sem,
    sq_recv_sem,
    z_buf,
    z_send_sem,
    z_recv_sem,
    term_buf,
    term_recv,
    term_send_sem,
    term_recv_sem,
    x_send_sem,
    x_recv_sem,
    pick,
    carried,
    drive_high,
    drive_low,
    mix_cat,
    base,
):
    i = lax.axis_index("dp")
    j = lax.axis_index("tp")
    layers, mine, groups, width = state.shape
    half = width // 2
    rows, local_d = x_buf.shape[1:]
    chans = w_out.shape[1]
    chunk = rows // n_tp
    per_block = mine // chunk
    channel_group = chans // groups

    dp_steps = [(0, 1)] + [
        (d, e) for d in (1, n_dp // 2 - 1, 2) for e in (0, 1)
    ]

    def dp_peer(step):
        d, e = step
        return lax.rem(lax.div(i, 2) + d, n_dp // 2) * 2 + lax.rem(lax.rem(i, 2) + e, 2)

    side = 1 - 2 * lax.rem(j, 2)
    far = n_tp // 2
    hub = far - 2
    tree = {o: o - sign(o) * step_to_hub(o) for o in range(1 - far, far) if o}
    children = {p: [o for o in tree if tree[o] == p] for p in [0, *tree]}
    by_reach = sorted(tree, key=lambda o: (-abs(o), o))
    leaves = [o for o in by_reach if not children[o]]
    hubs = [o for o in by_reach if children[o]]

    def at_offset(o):
        return lax.rem(j + o + n_tp, n_tp)

    barrier = pltpu.get_barrier_semaphore()
    for step in dp_steps:
        pl.semaphore_signal(barrier, inc=1, device_id={"dp": dp_peer(step)}, device_id_type=MESH)
    tp_greeted = sorted({(o - tree[o]) % n_tp for o in tree} | {2, n_tp - 2})
    for step in tp_greeted:
        pl.semaphore_signal(barrier, inc=1, device_id={"tp": at_offset(step)}, device_id_type=MESH)

    loads = {}
    for n, (name, src, dst) in enumerate(
        [
            ("x", tokens_hbm, x_buf.at[0]),
            ("norm", norm_hbm, norm),
            ("w_in", w_in_hbm, w_cat.at[:, :, pl.ds(0, chans)]),
            ("w_gate", w_gate_hbm, w_cat.at[:, :, pl.ds(chans, chans)]),
            ("decay", decay_hbm, decay),
            ("state", state_hbm, state),
            ("rate", rate_hbm, rate),
            ("freq", freq_hbm, freq),
            ("b", b_hbm, b_mat),
            ("c", c_hbm, c_mat),
            ("feed", feed_hbm, feed),
            ("w_out", w_out_hbm, w_out),
        ]
    ):
        loads[name] = pltpu.make_async_copy(src, dst, local_sem.at[n])
        loads[name].start()

    lane = lax.broadcasted_iota(jnp.int32, (groups, width), 1)
    sub = lax.broadcasted_iota(jnp.int32, (groups, width), 0)
    low = lane < half
    col_group = lax.broadcasted_iota(jnp.int32, (groups, chans), 1) // channel_group
    own_group = col_group == lax.broadcasted_iota(jnp.int32, (groups, chans), 0)
    block_row = lax.broadcasted_iota(jnp.int32, (chans, chans), 0) // channel_group
    block_col = lax.broadcasted_iota(jnp.int32, (chans, chans), 1) // channel_group

    def by_group(ref, layer):
        out = jnp.zeros((groups, width), F32)
        for g in range(groups):
            pair = ref[layer : layer + 1, (g // 2) * width : (g // 2 + 1) * width]
            other = pltpu.roll(pair, half, 1)
            row = jnp.where(low[:1] if g % 2 == 0 else ~low[:1], pair, other)
            out = jnp.where(sub == g, row, out)
        return out

    def prepare(layer):
        dt = jnp.zeros((groups, width), F32)
        for g in range(groups):
            dt = jnp.where(sub == g, step_width[layer, g], dt)
        a_re = by_group(rate, layer)
        a_im = by_group(freq, layer)
        log_mag = -a_re * dt
        turn = a_im * dt
        magnitude = jnp.exp(log_mag)
        cosine = jnp.cos(turn)
        disc_re = magnitude * cosine
        disc_im = magnitude * jnp.sin(turn)
        half_sine = jnp.sin(0.5 * turn)
        numer_re = exp_less_one(log_mag, magnitude) * cosine - 2.0 * half_sine * half_sine
        denom = a_re * a_re + a_im * a_im
        drive_re = (-numer_re * a_re + disc_im * a_im) / denom
        drive_im = (-disc_im * a_re - numer_re * a_im) / denom
        disc_cross = jnp.where(low, -disc_im, disc_im)
        drive_cross = jnp.where(low, -drive_im, drive_im)

        b_l = b_mat[layer]
        drive = drive_re[:, None, :] * b_l + drive_cross[:, None, :] * pltpu.roll(b_l, half, 2)
        drive = drive.reshape(chans, width)
        high, rest = split_two(drive)
        drive_high[layer] = high
        drive_low[layer] = rest
        c_l = jnp.where(low[:1][None], c_mat[layer], -c_mat[layer]).reshape(chans, width)
        mix = jnp.where(block_row == block_col, contract_last(drive, c_l, HIGHEST), 0.0)
        high, rest = split_two(mix)
        mix_cat[layer, :chans] = high
        mix_cat[layer, chans:] = rest

        for r in range(mine):
            offset = lane - (lengths[r] - 1)
            found = jnp.zeros((groups, width), F32)
            for at in range(0, decay.shape[2], width):
                found = jnp.where(offset == -at, decay[layer, :, at : at + width], found)
            pick[r] = found
        extra = jnp.exp(jnp.sum(pick[...], axis=-1, keepdims=True))
        s = state[layer]
        kept = extra * (disc_re[None] * s + disc_cross[None] * pltpu.roll(s, half, 2))
        carried[layer] = kept
        read = contract_last(kept.reshape(mine * groups, width), c_l, HIGHEST)
        read = jnp.where(own_group[None], read.reshape(mine, groups, chans), 0.0)
        base[layer] = jnp.sum(read, axis=1)

    def send_part(layer, s):
        for src, dst, ssem, rsem in (
            (part_buf, part_recv, part_send_sem, part_recv_sem),
            (sq_buf, sq_recv, sq_send_sem, sq_recv_sem),
        ):
            pltpu.make_async_remote_copy(
                src_ref=src.at[layer, s],
                dst_ref=dst.at[layer, i],
                send_sem=ssem.at[layer, s],
                recv_sem=rsem.at[layer, i],
                device_id={"dp": s},
                device_id_type=MESH,
            ).start()

    ones = jnp.ones((8, 128), F32)

    def square_rows(x):
        x2 = x * x
        total = x2[:, 0:128]
        for k in range(1, local_d // 128):
            total = total + x2[:, k * 128 : (k + 1) * 128]
        return contract_last(ones, total, HIGHEST)

    def chunk_rows(t):
        return pl.ds(pl.multiple_of(t * chunk, chunk), chunk)

    def up(layer, o):
        hop = 2 * side if o == far else o - tree[o]
        owner = at_offset(-o)
        return pltpu.make_async_remote_copy(
            src_ref=term_buf.at[layer, owner],
            dst_ref=term_recv.at[layer, o % n_tp],
            send_sem=term_send_sem.at[layer, o % n_tp],
            recv_sem=term_recv_sem.at[layer, o % n_tp],
            device_id={"tp": at_offset(-hop)},
            device_id_type=MESH,
        )

    arrived = up

    def down(layer, o, c):
        owner = chunk_rows(at_offset(-o))
        slot = lax.rem(c + n_tp, n_tp)
        return pltpu.make_async_remote_copy(
            src_ref=x_buf.at[layer + 1, owner],
            dst_ref=x_buf.at[layer + 1, owner],
            send_sem=x_send_sem.at[layer, slot],
            recv_sem=x_recv_sem.at[layer, slot],
            device_id={"tp": at_offset(c - o)},
            device_id_type=MESH,
        )

    def landed(layer, o):
        owner = chunk_rows(at_offset(-o))
        slot = lax.rem(o + n_tp, n_tp)
        return pltpu.make_async_remote_copy(
            src_ref=x_buf.at[layer + 1, owner],
            dst_ref=x_buf.at[layer + 1, owner],
            send_sem=x_send_sem.at[layer, slot],
            recv_sem=x_recv_sem.at[layer, slot],
            device_id={"tp": at_offset(1)},
            device_id_type=MESH,
        )


    loads["x"].wait()
    loads["norm"].wait()
    x = x_buf[0].astype(F32)
    scaled = (x * norm[0:1, :]).astype(BF16)
    squares = square_rows(x)
    for s in range(n_dp):
        sq_buf[0, s, :, pl.ds(0, mine)] = squares[:, s * mine : (s + 1) * mine]
    loads["w_in"].wait()
    loads["w_gate"].wait()
    part_buf[0] = (
        jnp.dot(scaled, w_cat[0], preferred_element_type=F32)
        .astype(BF16)
        .reshape(n_dp, mine, 2 * chans)
    )
    for name in ("decay", "state", "rate", "freq", "b", "c", "feed", "w_out"):
        loads[name].wait()
    pl.semaphore_wait(barrier, len(dp_steps) + len(tp_greeted))
    for step in dp_steps:
        send_part(0, dp_peer(step))
    for layer in range(layers):
        prepare(layer)

    row_lane = lax.broadcasted_iota(jnp.int32, (mine, 128), 1)
    row_sub = lax.broadcasted_iota(jnp.int32, (mine, 128), 0)

    for layer in range(layers):
        total = part_buf[layer, i].astype(F32)
        sq = sq_buf[layer, i]
        for step in dp_steps:
            s = dp_peer(step)
            for src, dst, ssem, rsem in (
                (part_buf, part_recv, part_send_sem, part_recv_sem),
                (sq_buf, sq_recv, sq_send_sem, sq_recv_sem),
            ):
                pltpu.make_async_remote_copy(
                    src_ref=src.at[layer, s],
                    dst_ref=dst.at[layer, s],
                    send_sem=ssem.at[layer, s],
                    recv_sem=rsem.at[layer, s],
                    device_id={"dp": s},
                    device_id_type=MESH,
                ).wait_recv()
            total = total + part_recv[layer, s].astype(F32)
            sq = sq + sq_recv[layer, s]
        mean = jnp.sum(
            jnp.where(row_lane == row_sub, sq[0:1, :], 0.0), axis=1, keepdims=True
        ) / features
        scale = lax.rsqrt(mean + NORM_EPS)
        total = total * scale
        u = total[:, :chans].astype(BF16)
        gate = total[:, chans:].astype(BF16).astype(F32)
        u_f = u.astype(F32)
        read = base[layer] + jnp.dot(
            jnp.concatenate([u, u], axis=1), mix_cat[layer], preferred_element_type=F32
        )
        y = jax.nn.gelu(read + feed[layer : layer + 1, :] * u_f)
        z_buf[layer, i] = (y * jax.nn.sigmoid(gate)).astype(BF16)
        for step in dp_steps:
            s = dp_peer(step)
            pltpu.make_async_remote_copy(
                src_ref=z_buf.at[layer, i],
                dst_ref=z_buf.at[layer, i],
                send_sem=z_send_sem.at[layer, s],
                recv_sem=z_recv_sem.at[layer, i],
                device_id={"dp": s},
                device_id_type=MESH,
            ).start()

        for step in dp_steps:
            s = dp_peer(step)
            pltpu.make_async_remote_copy(
                src_ref=z_buf.at[layer, s],
                dst_ref=z_buf.at[layer, s],
                send_sem=z_send_sem.at[layer, s],
                recv_sem=z_recv_sem.at[layer, s],
                device_id={"dp": s},
                device_id_type=MESH,
            ).wait_recv()
        terms = jnp.dot(
            z_buf[layer].reshape(rows, chans), w_out[layer], preferred_element_type=F32
        )
        term_buf[layer] = terms.astype(BF16).reshape(n_tp, chunk, local_d)

        up(layer, far).start()
        for o in leaves:
            up(layer, o).start()

        spread = jnp.where(own_group[None], u_f[:, None, :], 0.0).astype(BF16)
        spread = spread.reshape(mine * groups, chans)
        driven = jnp.dot(spread, drive_high[layer], preferred_element_type=F32) + jnp.dot(
            spread, drive_low[layer], preferred_element_type=F32
        )
        carried[layer] = carried[layer] + driven.reshape(mine, groups, width)
        pltpu.make_async_copy(carried.at[layer], state_out.at[layer], out_sem.at[layer]).start()

        arrived(layer, far).wait_recv()
        for o in hubs:
            owner = at_offset(-o)
            total = term_buf[layer, owner].astype(F32)
            for c in children[o]:
                arrived(layer, c).wait_recv()
                total = total + term_recv[layer, c % n_tp].astype(F32)
            if abs(o) == hub:
                last = term_recv[layer, far].astype(F32)
                total = total + jnp.where(side * o > 0, last, 0.0)
            term_buf[layer, owner] = total.astype(BF16)
            up(layer, o).start()
        total = term_buf[layer, j].astype(F32)
        for o in sorted(children[0], key=abs):
            arrived(layer, o).wait_recv()
            total = total + term_recv[layer, o % n_tp].astype(F32)
        at = chunk_rows(j)
        branch = total.astype(BF16).astype(F32)
        x_buf[layer + 1, at, :] = (x_buf[layer, at, :].astype(F32) + branch).astype(BF16)

        for c in sorted(children[0], key=lambda o: -abs(o)):
            down(layer, 0, c).start()
        for o in sorted(hubs, key=abs):
            landed(layer, o).wait_recv()
            for c in children[o]:
                down(layer, o, c).start()
        down(layer, hub * side, far * side).start()

        if layer + 1 < layers:
            order = [0]
            for d in range(1, n_dp // 2 + 1):
                order.append(d)
                if n_dp - d != d:
                    order.append(n_dp - d)
            for d in order:
                s = lax.rem(lax.div(j, per_block) + d, n_dp)
                for k in range(per_block):
                    t = s * per_block + k
                    o = lax.rem(j - t + n_tp, n_tp)
                    ready = o != 0
                    for h in hubs:
                        ready = ready & (o != h % n_tp)
                    pl.when(ready)(lambda o=o: landed(layer, o).wait_recv())
                piece = pl.ds(pl.multiple_of(s * mine, mine), mine)
                x = x_buf[layer + 1, piece, :].astype(F32)
                scaled = (x * norm[layer + 1 : layer + 2, :]).astype(BF16)
                sq_buf[layer + 1, s, :, pl.ds(0, mine)] = square_rows(x)
                part_buf[layer + 1, s] = jnp.dot(
                    scaled, w_cat[layer + 1], preferred_element_type=F32
                ).astype(BF16)
                pl.when(s != i)(functools.partial(send_part, layer + 1, s))
        else:
            for o in [*leaves, far]:
                landed(layer, o).wait_recv()
            pltpu.make_async_copy(x_buf.at[layers], tokens_out, out_sem.at[layers]).start()

    for layer in range(layers):
        for step in dp_steps:
            s = dp_peer(step)
            for src, dst, ssem, rsem in (
                (part_buf, part_recv, part_send_sem, part_recv_sem),
                (sq_buf, sq_recv, sq_send_sem, sq_recv_sem),
            ):
                pltpu.make_async_remote_copy(
                    src_ref=src.at[layer, s],
                    dst_ref=dst.at[layer, i],
                    send_sem=ssem.at[layer, s],
                    recv_sem=rsem.at[layer, i],
                    device_id={"dp": s},
                    device_id_type=MESH,
                ).wait_send()
            pltpu.make_async_remote_copy(
                src_ref=z_buf.at[layer, i],
                dst_ref=z_buf.at[layer, i],
                send_sem=z_send_sem.at[layer, s],
                recv_sem=z_recv_sem.at[layer, i],
                device_id={"dp": s},
                device_id_type=MESH,
            ).wait_send()
        for o in [*tree, far]:
            up(layer, o).wait_send()
        for o in tree:
            down(layer, tree[o], o).wait_send()
        down(layer, hub * side, far * side).wait_send()
        pltpu.make_async_copy(carried.at[layer], state_out.at[layer], out_sem.at[layer]).wait()
    pltpu.make_async_copy(x_buf.at[layers], tokens_out, out_sem.at[layers]).wait()


def on_device(
    n_dp,
    n_tp,
    tokens,
    sequence_lengths,
    recurrent_state,
    norm_weight,
    input_weight,
    gate_weight,
    output_weight,
    negated_real_rate,
    frequency,
    discrete_step,
    group_input_matrix,
    group_output_matrix,
    feedthrough_weight,
    extra_log_decay,
):
    layers, mine, groups, width = recurrent_state.shape
    rows, local_d = tokens.shape
    chans = output_weight.shape[1]
    chunk = rows // n_tp
    smem = pl.BlockSpec(memory_space=pltpu.SMEM)
    hbm = pl.BlockSpec(memory_space=pl.ANY)
    dma = pltpu.SemaphoreType.DMA
    like = lambda a: pltpu.VMEM(a.shape, a.dtype)
    scratch = [
        pltpu.VMEM((layers + 1, rows, local_d), BF16),
        like(norm_weight),
        pltpu.VMEM((layers, local_d, 2 * chans), BF16),
        like(output_weight),
        like(extra_log_decay),
        like(recurrent_state),
        like(negated_real_rate),
        like(frequency),
        like(group_input_matrix),
        like(group_output_matrix),
        like(feedthrough_weight),
        dma((12,)),
        dma((layers + 1,)),
        pltpu.VMEM((layers, n_dp, mine, 2 * chans), BF16),
        pltpu.VMEM((layers, n_dp, mine, 2 * chans), BF16),
        dma((layers, n_dp)),
        dma((layers, n_dp)),
        pltpu.VMEM((layers, n_dp, 8, 128), F32),
        pltpu.VMEM((layers, n_dp, 8, 128), F32),
        dma((layers, n_dp)),
        dma((layers, n_dp)),
        pltpu.VMEM((layers, n_dp, mine, chans), BF16),
        dma((layers, n_dp)),
        dma((layers, n_dp)),
        pltpu.VMEM((layers, n_tp, chunk, local_d), BF16),
        pltpu.VMEM((layers, n_tp, chunk, local_d), BF16),
        dma((layers, n_tp)),
        dma((layers, n_tp)),
        dma((layers, n_tp)),
        dma((layers, n_tp)),
        pltpu.VMEM((mine, groups, width), F32),
        pltpu.VMEM((layers, mine, groups, width), F32),
        pltpu.VMEM((layers, chans, width), BF16),
        pltpu.VMEM((layers, chans, width), BF16),
        pltpu.VMEM((layers, 2 * chans, chans), BF16),
        pltpu.VMEM((layers, mine, chans), F32),
    ]
    return pl.pallas_call(
        functools.partial(kernel, n_dp, n_tp, n_dp * local_d),
        out_shape=(
            jax.ShapeDtypeStruct(tokens.shape, tokens.dtype),
            jax.ShapeDtypeStruct(recurrent_state.shape, recurrent_state.dtype),
        ),
        in_specs=[smem, smem] + [hbm] * 12,
        out_specs=(hbm, hbm),
        scratch_shapes=scratch,
        compiler_params=pltpu.CompilerParams(collective_id=0, has_side_effects=True),
    )(
        sequence_lengths,
        discrete_step,
        tokens,
        norm_weight,
        input_weight,
        gate_weight,
        extra_log_decay,
        recurrent_state,
        negated_real_rate,
        frequency,
        group_input_matrix,
        group_output_matrix,
        feedthrough_weight,
        output_weight,
    )


def solution(mesh):
    in_specs = (
        P("grp", "dp"),
        P(("grp", "dp")),
        P(None, ("grp", "dp"), "tp", None),
        P(None, "dp"),
        P(None, "dp", "tp"),
        P(None, "dp", "tp"),
        P(None, "tp", "dp"),
        P(None, "tp"),
        P(None, "tp"),
        P(None, "tp"),
        P(None, "tp", None, None),
        P(None, "tp", None, None),
        P(None, "tp"),
        P(None, "tp", None),
    )
    out_specs = (P("grp", "dp"), P(None, ("grp", "dp"), "tp", None))
    return jax.shard_map(
        functools.partial(on_device, mesh.shape["dp"], mesh.shape["tp"]),
        mesh=mesh,
        in_specs=in_specs,
        out_specs=out_specs,
        check_vma=False,
    )
```

```python
import functools

import jax
import jax.numpy as jnp
from jax import lax
from jax.experimental import pallas as pl
from jax.experimental.pallas import tpu as pltpu
from jax.sharding import PartitionSpec as P

NORM_EPS = 1e-06
HIGHEST = lax.Precision.HIGHEST
F32 = jnp.float32
BF16 = jnp.bfloat16
MESH = pl.DeviceIdType.MESH


def contract_last(a, b, precision=None):
    return lax.dot_general(
        a, b, (((1,), (1,)), ((), ())), precision=precision, preferred_element_type=F32
    )


def split_two(a):
    high = a.astype(BF16)
    return high, (a - high.astype(F32)).astype(BF16)


def exp_less_one(x, exp_x):
    series = jnp.full_like(x, 1.0 / 3628800.0)
    for factor in (362880.0, 40320.0, 5040.0, 720.0, 120.0, 24.0, 6.0, 2.0, 1.0):
        series = series * x + 1.0 / factor
    return jnp.where(jnp.abs(x) < 0.6, series * x, exp_x - 1.0)


def sign(o):
    return 1 if o > 0 else -1


def step_to_hub(o):
    near = (abs(o) + 1) // 3 * 3
    return abs(o) if near in (0, abs(o)) else abs(o) - near


def kernel(
    n_dp,
    n_tp,
    features,
    lengths_hbm,
    step_hbm,
    tokens_hbm,
    norm_hbm,
    w_in_hbm,
    w_gate_hbm,
    decay_hbm,
    state_hbm,
    rate_hbm,
    freq_hbm,
    b_hbm,
    c_hbm,
    feed_hbm,
    w_out_hbm,
    tokens_out,
    state_out,
    lengths,
    step_width,
    x_buf,
    norm,
    w_cat,
    w_out,
    decay,
    state,
    rate,
    freq,
    b_mat,
    c_mat,
    feed,
    local_sem,
    out_sem,
    part_buf,
    part_recv,
    part_send_sem,
    part_recv_sem,
    sq_buf,
    sq_recv,
    sq_send_sem,
    sq_recv_sem,
    z_buf,
    z_send_sem,
    z_recv_sem,
    term_buf,
    term_recv,
    term_send_sem,
    term_recv_sem,
    x_send_sem,
    x_recv_sem,
    pick,
    carried,
    drive_high,
    drive_low,
    mix_cat,
    base,
):
    i = lax.axis_index("dp")
    j = lax.axis_index("tp")
    layers, mine, groups, width = state.shape
    half = width // 2
    rows, local_d = x_buf.shape[1:]
    chans = w_out.shape[1]
    chunk = rows // n_tp
    per_block = mine // chunk
    channel_group = chans // groups

    dp_steps = [(0, 1)] + [
        (d, e) for d in (1, n_dp // 2 - 1, 2) for e in (0, 1)
    ]

    def dp_peer(step):
        d, e = step
        return lax.rem(lax.div(i, 2) + d, n_dp // 2) * 2 + lax.rem(lax.rem(i, 2) + e, 2)

    side = 1 - 2 * lax.rem(j, 2)
    far = n_tp // 2
    hub = far - 2
    tree = {o: o - sign(o) * step_to_hub(o) for o in range(1 - far, far) if o}
    children = {p: [o for o in tree if tree[o] == p] for p in [0, *tree]}
    by_reach = sorted(tree, key=lambda o: (-abs(o), o))
    leaves = [o for o in by_reach if not children[o]]
    hubs = [o for o in by_reach if children[o]]

    def at_offset(o):
        return lax.rem(j + o + n_tp, n_tp)

    loads = {}
    for n, (name, src, dst) in enumerate(
        [
            ("x", tokens_hbm, x_buf.at[0]),
            ("norm", norm_hbm, norm),
            ("w_in", w_in_hbm, w_cat.at[:, :, pl.ds(0, chans)]),
            ("w_gate", w_gate_hbm, w_cat.at[:, :, pl.ds(chans, chans)]),
            ("decay", decay_hbm, decay),
            ("state", state_hbm, state),
            ("rate", rate_hbm, rate),
            ("freq", freq_hbm, freq),
            ("b", b_hbm, b_mat),
            ("c", c_hbm, c_mat),
            ("feed", feed_hbm, feed),
            ("lengths", lengths_hbm, lengths),
            ("step", step_hbm, step_width),
            ("w_out", w_out_hbm, w_out),
        ]
    ):
        loads[name] = pltpu.make_async_copy(src, dst, local_sem.at[n])
    for name in ("x", "norm", "w_in", "w_gate"):
        loads[name].start()

    barrier = pltpu.get_barrier_semaphore()
    for step in dp_steps:
        pl.semaphore_signal(barrier, inc=1, device_id={"dp": dp_peer(step)}, device_id_type=MESH)
    tp_greeted = sorted({(o - tree[o]) % n_tp for o in tree} | {2, n_tp - 2})
    for step in tp_greeted:
        pl.semaphore_signal(barrier, inc=1, device_id={"tp": at_offset(step)}, device_id_type=MESH)

    later = [name for name in loads if name not in ("x", "norm", "w_in", "w_gate")]
    for name in later:
        loads[name].start()

    lane = lax.broadcasted_iota(jnp.int32, (groups, width), 1)
    sub = lax.broadcasted_iota(jnp.int32, (groups, width), 0)
    low = lane < half
    col_group = lax.broadcasted_iota(jnp.int32, (groups, chans), 1) // channel_group
    own_group = col_group == lax.broadcasted_iota(jnp.int32, (groups, chans), 0)
    block_row = lax.broadcasted_iota(jnp.int32, (chans, chans), 0) // channel_group
    block_col = lax.broadcasted_iota(jnp.int32, (chans, chans), 1) // channel_group

    def by_group(ref, layer):
        out = jnp.zeros((groups, width), F32)
        for g in range(groups):
            pair = ref[layer : layer + 1, (g // 2) * width : (g // 2 + 1) * width]
            other = pltpu.roll(pair, half, 1)
            row = jnp.where(low[:1] if g % 2 == 0 else ~low[:1], pair, other)
            out = jnp.where(sub == g, row, out)
        return out

    def prepare(layer):
        dt = jnp.zeros((groups, width), F32)
        for g in range(groups):
            dt = jnp.where(sub == g, step_width[layer, g], dt)
        a_re = by_group(rate, layer)
        a_im = by_group(freq, layer)
        log_mag = -a_re * dt
        turn = a_im * dt
        magnitude = jnp.exp(log_mag)
        cosine = jnp.cos(turn)
        disc_re = magnitude * cosine
        disc_im = magnitude * jnp.sin(turn)
        half_sine = jnp.sin(0.5 * turn)
        numer_re = exp_less_one(log_mag, magnitude) * cosine - 2.0 * half_sine * half_sine
        denom = a_re * a_re + a_im * a_im
        drive_re = (-numer_re * a_re + disc_im * a_im) / denom
        drive_im = (-disc_im * a_re - numer_re * a_im) / denom
        disc_cross = jnp.where(low, -disc_im, disc_im)
        drive_cross = jnp.where(low, -drive_im, drive_im)

        b_l = b_mat[layer]
        drive = drive_re[:, None, :] * b_l + drive_cross[:, None, :] * pltpu.roll(b_l, half, 2)
        drive = drive.reshape(chans, width)
        high, rest = split_two(drive)
        drive_high[layer] = high
        drive_low[layer] = rest
        c_l = jnp.where(low[:1][None], c_mat[layer], -c_mat[layer]).reshape(chans, width)
        mix = jnp.where(block_row == block_col, contract_last(drive, c_l, HIGHEST), 0.0)
        high, rest = split_two(mix)
        mix_cat[layer, :chans] = high
        mix_cat[layer, chans:] = rest

        for r in range(mine):
            offset = lane - (lengths[r] - 1)
            found = jnp.zeros((groups, width), F32)
            for at in range(0, decay.shape[2], width):
                found = jnp.where(offset == -at, decay[layer, :, at : at + width], found)
            pick[r] = found
        extra = jnp.exp(jnp.sum(pick[...], axis=-1, keepdims=True))
        s = state[layer]
        kept = extra * (disc_re[None] * s + disc_cross[None] * pltpu.roll(s, half, 2))
        carried[layer] = kept
        read = contract_last(kept.reshape(mine * groups, width), c_l, HIGHEST)
        read = jnp.where(own_group[None], read.reshape(mine, groups, chans), 0.0)
        base[layer] = jnp.sum(read, axis=1)

    def send_part(layer, s):
        for src, dst, ssem, rsem in (
            (part_buf, part_recv, part_send_sem, part_recv_sem),
            (sq_buf, sq_recv, sq_send_sem, sq_recv_sem),
        ):
            pltpu.make_async_remote_copy(
                src_ref=src.at[layer, s],
                dst_ref=dst.at[layer, i],
                send_sem=ssem.at[layer, s],
                recv_sem=rsem.at[layer, i],
                device_id={"dp": s},
                device_id_type=MESH,
            ).start()

    ones = jnp.ones((8, 128), F32)

    def square_rows(x):
        x2 = x * x
        total = x2[:, 0:128]
        for k in range(1, local_d // 128):
            total = total + x2[:, k * 128 : (k + 1) * 128]
        return contract_last(ones, total, HIGHEST)

    def chunk_rows(t):
        return pl.ds(pl.multiple_of(t * chunk, chunk), chunk)

    def up(layer, o):
        hop = 2 * side if o == far else o - tree[o]
        owner = at_offset(-o)
        return pltpu.make_async_remote_copy(
            src_ref=term_buf.at[layer, owner],
            dst_ref=term_recv.at[layer, o % n_tp],
            send_sem=term_send_sem.at[layer, o % n_tp],
            recv_sem=term_recv_sem.at[layer, o % n_tp],
            device_id={"tp": at_offset(-hop)},
            device_id_type=MESH,
        )

    arrived = up

    def down(layer, o, c):
        owner = chunk_rows(at_offset(-o))
        slot = lax.rem(c + n_tp, n_tp)
        return pltpu.make_async_remote_copy(
            src_ref=x_buf.at[layer + 1, owner],
            dst_ref=x_buf.at[layer + 1, owner],
            send_sem=x_send_sem.at[layer, slot],
            recv_sem=x_recv_sem.at[layer, slot],
            device_id={"tp": at_offset(c - o)},
            device_id_type=MESH,
        )

    def landed(layer, o):
        owner = chunk_rows(at_offset(-o))
        slot = lax.rem(o + n_tp, n_tp)
        return pltpu.make_async_remote_copy(
            src_ref=x_buf.at[layer + 1, owner],
            dst_ref=x_buf.at[layer + 1, owner],
            send_sem=x_send_sem.at[layer, slot],
            recv_sem=x_recv_sem.at[layer, slot],
            device_id={"tp": at_offset(1)},
            device_id_type=MESH,
        )


    loads["x"].wait()
    loads["norm"].wait()
    x = x_buf[0].astype(F32)
    scaled = (x * norm[0:1, :]).astype(BF16)
    squares = square_rows(x)
    for s in range(n_dp):
        sq_buf[0, s, :, pl.ds(0, mine)] = squares[0:1, s * mine : (s + 1) * mine]
    loads["w_in"].wait()
    loads["w_gate"].wait()
    part_buf[0] = (
        jnp.dot(scaled, w_cat[0], preferred_element_type=F32)
        .astype(BF16)
        .reshape(n_dp, mine, 2 * chans)
    )
    pl.semaphore_wait(barrier, len(dp_steps) + len(tp_greeted))
    for step in dp_steps:
        send_part(0, dp_peer(step))
    for name in later:
        loads[name].wait()
    for layer in range(layers):
        prepare(layer)

    row_lane = lax.broadcasted_iota(jnp.int32, (mine, 128), 1)
    row_sub = lax.broadcasted_iota(jnp.int32, (mine, 128), 0)

    for layer in range(layers):
        total = part_buf[layer, i].astype(F32)
        sq = sq_buf[layer, i]
        for step in dp_steps:
            s = dp_peer(step)
            for src, dst, ssem, rsem in (
                (part_buf, part_recv, part_send_sem, part_recv_sem),
                (sq_buf, sq_recv, sq_send_sem, sq_recv_sem),
            ):
                pltpu.make_async_remote_copy(
                    src_ref=src.at[layer, s],
                    dst_ref=dst.at[layer, s],
                    send_sem=ssem.at[layer, s],
                    recv_sem=rsem.at[layer, s],
                    device_id={"dp": s},
                    device_id_type=MESH,
                ).wait_recv()
            total = total + part_recv[layer, s].astype(F32)
            sq = sq + sq_recv[layer, s]
        mean = jnp.sum(
            jnp.where(row_lane == row_sub, sq[0:1, :], 0.0), axis=1, keepdims=True
        ) / features
        scale = lax.rsqrt(mean + NORM_EPS)
        total = total * scale
        u = total[:, :chans].astype(BF16)
        gate = total[:, chans:].astype(BF16).astype(F32)
        u_f = u.astype(F32)
        read = base[layer] + jnp.dot(
            jnp.concatenate([u, u], axis=1), mix_cat[layer], preferred_element_type=F32
        )
        y = jax.nn.gelu(read + feed[layer : layer + 1, :] * u_f)
        z_buf[layer, i] = (y * jax.nn.sigmoid(gate)).astype(BF16)
        for step in dp_steps:
            s = dp_peer(step)
            pltpu.make_async_remote_copy(
                src_ref=z_buf.at[layer, i],
                dst_ref=z_buf.at[layer, i],
                send_sem=z_send_sem.at[layer, s],
                recv_sem=z_recv_sem.at[layer, i],
                device_id={"dp": s},
                device_id_type=MESH,
            ).start()

        for step in dp_steps:
            s = dp_peer(step)
            pltpu.make_async_remote_copy(
                src_ref=z_buf.at[layer, s],
                dst_ref=z_buf.at[layer, s],
                send_sem=z_send_sem.at[layer, s],
                recv_sem=z_recv_sem.at[layer, s],
                device_id={"dp": s},
                device_id_type=MESH,
            ).wait_recv()
        terms = jnp.dot(
            z_buf[layer].reshape(rows, chans), w_out[layer], preferred_element_type=F32
        )
        term_buf[layer] = terms.astype(BF16).reshape(n_tp, chunk, local_d)

        up(layer, far).start()
        for o in leaves:
            up(layer, o).start()

        spread = jnp.where(own_group[None], u_f[:, None, :], 0.0).astype(BF16)
        spread = spread.reshape(mine * groups, chans)
        driven = jnp.dot(spread, drive_high[layer], preferred_element_type=F32) + jnp.dot(
            spread, drive_low[layer], preferred_element_type=F32
        )
        state_out[layer] = carried[layer] + driven.reshape(mine, groups, width)

        arrived(layer, far).wait_recv()
        for o in hubs:
            owner = at_offset(-o)
            total = term_buf[layer, owner].astype(F32)
            for c in children[o]:
                arrived(layer, c).wait_recv()
                total = total + term_recv[layer, c % n_tp].astype(F32)
            if abs(o) == hub:
                last = term_recv[layer, far].astype(F32)
                total = total + jnp.where(side * o > 0, last, 0.0)
            term_buf[layer, owner] = total.astype(BF16)
            up(layer, o).start()
        total = term_buf[layer, j].astype(F32)
        for o in sorted(children[0], key=abs):
            arrived(layer, o).wait_recv()
            total = total + term_recv[layer, o % n_tp].astype(F32)
        at = chunk_rows(j)
        branch = total.astype(BF16).astype(F32)
        x_buf[layer + 1, at, :] = (x_buf[layer, at, :].astype(F32) + branch).astype(BF16)

        for c in sorted(children[0], key=lambda o: -abs(o)):
            down(layer, 0, c).start()
        for o in sorted(hubs, key=abs):
            landed(layer, o).wait_recv()
            for c in children[o]:
                down(layer, o, c).start()
        down(layer, hub * side, far * side).start()

        if layer + 1 < layers:
            order = [0]
            for d in range(1, n_dp // 2 + 1):
                order.append(d)
                if n_dp - d != d:
                    order.append(n_dp - d)
            for d in order:
                s = lax.rem(lax.div(j, per_block) + d, n_dp)
                for k in range(per_block):
                    t = s * per_block + k
                    o = lax.rem(j - t + n_tp, n_tp)
                    ready = o != 0
                    for h in hubs:
                        ready = ready & (o != h % n_tp)
                    pl.when(ready)(lambda o=o: landed(layer, o).wait_recv())
                piece = pl.ds(pl.multiple_of(s * mine, mine), mine)
                x = x_buf[layer + 1, piece, :].astype(F32)
                scaled = (x * norm[layer + 1 : layer + 2, :]).astype(BF16)
                sq_buf[layer + 1, s, :, pl.ds(0, mine)] = square_rows(x)[0:1]
                part_buf[layer + 1, s] = jnp.dot(
                    scaled, w_cat[layer + 1], preferred_element_type=F32
                ).astype(BF16)
                pl.when(s != i)(functools.partial(send_part, layer + 1, s))
        else:
            for o in [*leaves, far]:
                landed(layer, o).wait_recv()
            tokens_out[...] = x_buf[layers]

    for layer in range(layers):
        for step in dp_steps:
            s = dp_peer(step)
            for src, dst, ssem, rsem in (
                (part_buf, part_recv, part_send_sem, part_recv_sem),
                (sq_buf, sq_recv, sq_send_sem, sq_recv_sem),
            ):
                pltpu.make_async_remote_copy(
                    src_ref=src.at[layer, s],
                    dst_ref=dst.at[layer, i],
                    send_sem=ssem.at[layer, s],
                    recv_sem=rsem.at[layer, i],
                    device_id={"dp": s},
                    device_id_type=MESH,
                ).wait_send()
            pltpu.make_async_remote_copy(
                src_ref=z_buf.at[layer, i],
                dst_ref=z_buf.at[layer, i],
                send_sem=z_send_sem.at[layer, s],
                recv_sem=z_recv_sem.at[layer, i],
                device_id={"dp": s},
                device_id_type=MESH,
            ).wait_send()
        for o in [*tree, far]:
            up(layer, o).wait_send()
        for o in tree:
            down(layer, tree[o], o).wait_send()
        down(layer, hub * side, far * side).wait_send()


def on_device(
    n_dp,
    n_tp,
    tokens,
    sequence_lengths,
    recurrent_state,
    norm_weight,
    input_weight,
    gate_weight,
    output_weight,
    negated_real_rate,
    frequency,
    discrete_step,
    group_input_matrix,
    group_output_matrix,
    feedthrough_weight,
    extra_log_decay,
):
    layers, mine, groups, width = recurrent_state.shape
    rows, local_d = tokens.shape
    chans = output_weight.shape[1]
    chunk = rows // n_tp
    hbm = pl.BlockSpec(memory_space=pltpu.HBM)
    dma = pltpu.SemaphoreType.DMA
    in_hbm = lambda a: pltpu.with_memory_space_constraint(a, pltpu.HBM)
    like = lambda a: pltpu.VMEM(a.shape, a.dtype)
    scratch = [
        pltpu.SMEM(sequence_lengths.shape, sequence_lengths.dtype),
        pltpu.SMEM(discrete_step.shape, discrete_step.dtype),
        pltpu.VMEM((layers + 1, rows, local_d), BF16),
        like(norm_weight),
        pltpu.VMEM((layers, local_d, 2 * chans), BF16),
        like(output_weight),
        like(extra_log_decay),
        like(recurrent_state),
        like(negated_real_rate),
        like(frequency),
        like(group_input_matrix),
        like(group_output_matrix),
        like(feedthrough_weight),
        dma((14,)),
        dma((layers + 1,)),
        pltpu.VMEM((layers, n_dp, mine, 2 * chans), BF16),
        pltpu.VMEM((layers, n_dp, mine, 2 * chans), BF16),
        dma((layers, n_dp)),
        dma((layers, n_dp)),
        pltpu.VMEM((layers, n_dp, 1, 128), F32),
        pltpu.VMEM((layers, n_dp, 1, 128), F32),
        dma((layers, n_dp)),
        dma((layers, n_dp)),
        pltpu.VMEM((layers, n_dp, mine, chans), BF16),
        dma((layers, n_dp)),
        dma((layers, n_dp)),
        pltpu.VMEM((layers, n_tp, chunk, local_d), BF16),
        pltpu.VMEM((layers, n_tp, chunk, local_d), BF16),
        dma((layers, n_tp)),
        dma((layers, n_tp)),
        dma((layers, n_tp)),
        dma((layers, n_tp)),
        pltpu.VMEM((mine, groups, width), F32),
        pltpu.VMEM((layers, mine, groups, width), F32),
        pltpu.VMEM((layers, chans, width), BF16),
        pltpu.VMEM((layers, chans, width), BF16),
        pltpu.VMEM((layers, 2 * chans, chans), BF16),
        pltpu.VMEM((layers, mine, chans), F32),
    ]
    return pl.pallas_call(
        functools.partial(kernel, n_dp, n_tp, n_dp * local_d),
        out_shape=(
            jax.ShapeDtypeStruct(tokens.shape, tokens.dtype),
            jax.ShapeDtypeStruct(recurrent_state.shape, recurrent_state.dtype),
        ),
        in_specs=[hbm] * 14,
        out_specs=(pl.BlockSpec(memory_space=pltpu.VMEM),) * 2,
        scratch_shapes=scratch,
        compiler_params=pltpu.CompilerParams(collective_id=0, has_side_effects=True, vmem_limit_bytes=16 * 2**20),
    )(
        in_hbm(sequence_lengths),
        in_hbm(discrete_step),
        in_hbm(tokens),
        in_hbm(norm_weight),
        in_hbm(input_weight),
        in_hbm(gate_weight),
        in_hbm(extra_log_decay),
        in_hbm(recurrent_state),
        in_hbm(negated_real_rate),
        in_hbm(frequency),
        in_hbm(group_input_matrix),
        in_hbm(group_output_matrix),
        in_hbm(feedthrough_weight),
        in_hbm(output_weight),
    )


def solution(mesh):
    in_specs = (
        P("grp", "dp"),
        P(("grp", "dp")),
        P(None, ("grp", "dp"), "tp", None),
        P(None, "dp"),
        P(None, "dp", "tp"),
        P(None, "dp", "tp"),
        P(None, "tp", "dp"),
        P(None, "tp"),
        P(None, "tp"),
        P(None, "tp"),
        P(None, "tp", None, None),
        P(None, "tp", None, None),
        P(None, "tp"),
        P(None, "tp", None),
    )
    out_specs = (P("grp", "dp"), P(None, ("grp", "dp"), "tp", None))
    return jax.shard_map(
        functools.partial(on_device, mesh.shape["dp"], mesh.shape["tp"]),
        mesh=mesh,
        in_specs=in_specs,
        out_specs=out_specs,
        check_vma=False,
    )
```

```python
import functools

import jax
import jax.numpy as jnp
from jax import lax
from jax.experimental import pallas as pl
from jax.experimental.pallas import tpu as pltpu
from jax.sharding import PartitionSpec as P

NORM_EPS = 1e-06
HIGHEST = lax.Precision.HIGHEST
F32 = jnp.float32
BF16 = jnp.bfloat16
MESH = pl.DeviceIdType.MESH


def contract_last(a, b, precision=None):
    return lax.dot_general(
        a, b, (((1,), (1,)), ((), ())), precision=precision, preferred_element_type=F32
    )


def split_two(a):
    high = a.astype(BF16)
    return high, (a - high.astype(F32)).astype(BF16)


def exp_less_one(x, exp_x):
    series = jnp.full_like(x, 1.0 / 3628800.0)
    for factor in (362880.0, 40320.0, 5040.0, 720.0, 120.0, 24.0, 6.0, 2.0, 1.0):
        series = series * x + 1.0 / factor
    return jnp.where(jnp.abs(x) < 0.6, series * x, exp_x - 1.0)


def sign(o):
    return 1 if o > 0 else -1


def step_to_hub(o):
    near = (abs(o) + 1) // 3 * 3
    return abs(o) if near in (0, abs(o)) else abs(o) - near


def kernel(
    n_dp,
    n_tp,
    features,
    lengths_hbm,
    step_hbm,
    tokens_hbm,
    norm_hbm,
    w_in_hbm,
    w_gate_hbm,
    decay_hbm,
    state_hbm,
    rate_hbm,
    freq_hbm,
    b_hbm,
    c_hbm,
    feed_hbm,
    w_out_hbm,
    tokens_out,
    state_out,
    lengths,
    step_width,
    x_buf,
    norm,
    w_cat,
    w_out,
    decay,
    state,
    rate,
    freq,
    b_mat,
    c_mat,
    feed,
    local_sem,
    out_sem,
    part_buf,
    part_recv,
    part_send_sem,
    part_recv_sem,
    sq_buf,
    sq_recv,
    sq_send_sem,
    sq_recv_sem,
    z_buf,
    z_send_sem,
    z_recv_sem,
    term_buf,
    term_recv,
    term_send_sem,
    term_recv_sem,
    x_send_sem,
    x_recv_sem,
    pick,
    carried,
    drive_high,
    drive_low,
    mix_cat,
    base,
    relay,
):
    i = lax.axis_index("dp")
    j = lax.axis_index("tp")
    layers, mine, groups, width = state.shape
    half = width // 2
    rows, local_d = x_buf.shape[1:]
    chans = w_out.shape[1]
    chunk = rows // n_tp
    per_block = mine // chunk
    channel_group = chans // groups

    dp_steps = [(0, 1)] + [
        (d, e) for d in (1, n_dp // 2 - 1, n_dp // 4) for e in (0, 1)
    ]

    def dp_peer(step):
        d, e = step
        return lax.rem(lax.div(i, 2) + d, n_dp // 2) * 2 + lax.rem(lax.rem(i, 2) + e, 2)

    side = 1 - 2 * lax.rem(j, 2)
    far = n_tp // 2
    hub = far - 2
    tree = {o: o - sign(o) * step_to_hub(o) for o in range(1 - far, far) if o}
    children = {p: [o for o in tree if tree[o] == p] for p in [0, *tree]}
    by_reach = sorted(tree, key=lambda o: (-abs(o), o))
    leaves = [o for o in by_reach if not children[o]]
    hubs = [o for o in by_reach if children[o]]

    def at_offset(o):
        return lax.rem(j + o + n_tp, n_tp)

    loads = {}
    for n, (name, src, dst) in enumerate(
        [
            ("x", tokens_hbm, x_buf.at[0]),
            ("norm", norm_hbm, norm),
            ("w_in", w_in_hbm, w_cat.at[:, :, pl.ds(0, chans)]),
            ("w_gate", w_gate_hbm, w_cat.at[:, :, pl.ds(chans, chans)]),
            ("decay", decay_hbm, decay),
            ("state", state_hbm, state),
            ("rate", rate_hbm, rate),
            ("freq", freq_hbm, freq),
            ("b", b_hbm, b_mat),
            ("c", c_hbm, c_mat),
            ("feed", feed_hbm, feed),
            ("lengths", lengths_hbm, lengths),
            ("step", step_hbm, step_width),
            ("w_out", w_out_hbm, w_out),
        ]
    ):
        loads[name] = pltpu.make_async_copy(src, dst, local_sem.at[n])
    for name in ("x", "norm", "w_in", "w_gate"):
        loads[name].start()

    barrier = pltpu.get_barrier_semaphore()
    for step in dp_steps:
        pl.semaphore_signal(barrier, inc=1, device_id={"dp": dp_peer(step)}, device_id_type=MESH)
    tp_greeted = [o for o in (-3, 3, -2, 2, -1, 1)]
    for step in tp_greeted:
        pl.semaphore_signal(barrier, inc=1, device_id={"tp": at_offset(step)}, device_id_type=MESH)

    later = [name for name in loads if name not in ("x", "norm", "w_in", "w_gate")]
    for name in later:
        loads[name].start()

    lane = lax.broadcasted_iota(jnp.int32, (groups, width), 1)
    sub = lax.broadcasted_iota(jnp.int32, (groups, width), 0)
    low = lane < half
    col_group = lax.broadcasted_iota(jnp.int32, (groups, chans), 1) // channel_group
    own_group = col_group == lax.broadcasted_iota(jnp.int32, (groups, chans), 0)
    block_row = lax.broadcasted_iota(jnp.int32, (chans, chans), 0) // channel_group
    block_col = lax.broadcasted_iota(jnp.int32, (chans, chans), 1) // channel_group

    def by_group(ref, layer):
        out = jnp.zeros((groups, width), F32)
        for g in range(groups):
            pair = ref[layer : layer + 1, (g // 2) * width : (g // 2 + 1) * width]
            other = pltpu.roll(pair, half, 1)
            row = jnp.where(low[:1] if g % 2 == 0 else ~low[:1], pair, other)
            out = jnp.where(sub == g, row, out)
        return out

    def prepare(layer):
        dt = jnp.zeros((groups, width), F32)
        for g in range(groups):
            dt = jnp.where(sub == g, step_width[layer, g], dt)
        a_re = by_group(rate, layer)
        a_im = by_group(freq, layer)
        log_mag = -a_re * dt
        turn = a_im * dt
        magnitude = jnp.exp(log_mag)
        cosine = jnp.cos(turn)
        disc_re = magnitude * cosine
        disc_im = magnitude * jnp.sin(turn)
        half_sine = jnp.sin(0.5 * turn)
        numer_re = exp_less_one(log_mag, magnitude) * cosine - 2.0 * half_sine * half_sine
        denom = a_re * a_re + a_im * a_im
        drive_re = (-numer_re * a_re + disc_im * a_im) / denom
        drive_im = (-disc_im * a_re - numer_re * a_im) / denom
        disc_cross = jnp.where(low, -disc_im, disc_im)
        drive_cross = jnp.where(low, -drive_im, drive_im)

        b_l = b_mat[layer]
        drive = drive_re[:, None, :] * b_l + drive_cross[:, None, :] * pltpu.roll(b_l, half, 2)
        drive = drive.reshape(chans, width)
        high, rest = split_two(drive)
        drive_high[layer] = high
        drive_low[layer] = rest
        c_l = jnp.where(low[:1][None], c_mat[layer], -c_mat[layer]).reshape(chans, width)
        mix = jnp.where(block_row == block_col, contract_last(drive, c_l, HIGHEST), 0.0)
        high, rest = split_two(mix)
        mix_cat[layer, :chans] = high
        mix_cat[layer, chans:] = rest

        for r in range(mine):
            offset = lane - (lengths[r] - 1)
            found = jnp.zeros((groups, width), F32)
            for at in range(0, decay.shape[2], width):
                found = jnp.where(offset == -at, decay[layer, :, at : at + width], found)
            pick[r] = found
        extra = jnp.exp(jnp.sum(pick[...], axis=-1, keepdims=True))
        s = state[layer]
        kept = extra * (disc_re[None] * s + disc_cross[None] * pltpu.roll(s, half, 2))
        carried[layer] = kept
        read = contract_last(kept.reshape(mine * groups, width), c_l, HIGHEST)
        read = jnp.where(own_group[None], read.reshape(mine, groups, chans), 0.0)
        base[layer] = jnp.sum(read, axis=1)

    def send_part(layer, s):
        for src, dst, ssem, rsem in (
            (part_buf, part_recv, part_send_sem, part_recv_sem),
            (sq_buf, sq_recv, sq_send_sem, sq_recv_sem),
        ):
            pltpu.make_async_remote_copy(
                src_ref=src.at[layer, s],
                dst_ref=dst.at[layer, i],
                send_sem=ssem.at[layer, s],
                recv_sem=rsem.at[layer, i],
                device_id={"dp": s},
                device_id_type=MESH,
            ).start()

    def await_sends(layer):
        for step in dp_steps:
            s = dp_peer(step)
            for src, dst, ssem, rsem in (
                (part_buf, part_recv, part_send_sem, part_recv_sem),
                (sq_buf, sq_recv, sq_send_sem, sq_recv_sem),
            ):
                pltpu.make_async_remote_copy(
                    src_ref=src.at[layer, s],
                    dst_ref=dst.at[layer, i],
                    send_sem=ssem.at[layer, s],
                    recv_sem=rsem.at[layer, i],
                    device_id={"dp": s},
                    device_id_type=MESH,
                ).wait_send()
            pltpu.make_async_remote_copy(
                src_ref=z_buf.at[layer, i],
                dst_ref=z_buf.at[layer, i],
                send_sem=z_send_sem.at[layer, s],
                recv_sem=z_recv_sem.at[layer, i],
                device_id={"dp": s},
                device_id_type=MESH,
            ).wait_send()
        for o in [*tree, far]:
            up(layer, o).wait_send()
        for o in tree:
            down(layer, tree[o], o).wait_send()
        down(layer, hub * side, far * side).wait_send()

    ones = jnp.ones((8, 128), F32)

    def square_rows(x):
        x2 = x * x
        total = x2[:, 0:128]
        for k in range(1, local_d // 128):
            total = total + x2[:, k * 128 : (k + 1) * 128]
        return contract_last(ones, total, HIGHEST)

    def chunk_rows(t):
        return pl.ds(pl.multiple_of(t * chunk, chunk), chunk)

    def up(layer, o):
        hop = 2 * side if o == far else o - tree[o]
        owner = at_offset(-o)
        return pltpu.make_async_remote_copy(
            src_ref=term_buf.at[layer, owner],
            dst_ref=term_recv.at[layer, o % n_tp],
            send_sem=term_send_sem.at[layer, o % n_tp],
            recv_sem=term_recv_sem.at[layer, o % n_tp],
            device_id={"tp": at_offset(-hop)},
            device_id_type=MESH,
        )

    arrived = up

    def climb(layer, owner, o, past, reach):
        hop = (1 - 2 * past) * (reach - lax.div(reach + 1, 3) * 3)
        pltpu.make_async_remote_copy(
            src_ref=term_buf.at[layer, owner],
            dst_ref=term_recv.at[layer, o],
            send_sem=term_send_sem.at[layer, o],
            recv_sem=term_recv_sem.at[layer, o],
            device_id={"tp": at_offset(-hop)},
            device_id_type=MESH,
        ).start()

    def down(layer, o, c):
        owner = chunk_rows(at_offset(-o))
        slot = lax.rem(c + n_tp, n_tp)
        return pltpu.make_async_remote_copy(
            src_ref=x_buf.at[layer + 1, owner],
            dst_ref=x_buf.at[layer + 1, owner],
            send_sem=x_send_sem.at[layer, slot],
            recv_sem=x_recv_sem.at[layer, slot],
            device_id={"tp": at_offset(c - o)},
            device_id_type=MESH,
        )

    def landed(layer, o):
        owner = chunk_rows(at_offset(-o))
        slot = lax.rem(o + n_tp, n_tp)
        return pltpu.make_async_remote_copy(
            src_ref=x_buf.at[layer + 1, owner],
            dst_ref=x_buf.at[layer + 1, owner],
            send_sem=x_send_sem.at[layer, slot],
            recv_sem=x_recv_sem.at[layer, slot],
            device_id={"tp": at_offset(1)},
            device_id_type=MESH,
        )


    loads["x"].wait()
    loads["norm"].wait()
    x = x_buf[0].astype(F32)
    scaled = (x * norm[0:1, :]).astype(BF16)
    squares = square_rows(x)
    for s in range(n_dp):
        sq_buf[0, s, :, pl.ds(0, mine)] = squares[0:1, s * mine : (s + 1) * mine]
    loads["w_in"].wait()
    loads["w_gate"].wait()
    part_buf[0] = (
        jnp.dot(scaled, w_cat[0], preferred_element_type=F32)
        .astype(BF16)
        .reshape(n_dp, mine, 2 * chans)
    )
    pl.semaphore_wait(barrier, len(dp_steps) + len(tp_greeted))
    for step in (-hub // 2, hub // 2):
        pl.semaphore_signal(relay, inc=1, device_id={"tp": at_offset(step)}, device_id_type=MESH)
    for step in reversed(dp_steps):
        send_part(0, dp_peer(step))
    for name in later:
        loads[name].wait()
    for layer in range(layers):
        prepare(layer)

    row_lane = lax.broadcasted_iota(jnp.int32, (mine, 128), 1)
    row_sub = lax.broadcasted_iota(jnp.int32, (mine, 128), 0)

    for layer in range(layers):
        total = part_buf[layer, i].astype(F32)
        sq = sq_buf[layer, i]
        for step in dp_steps:
            s = dp_peer(step)
            for src, dst, ssem, rsem in (
                (part_buf, part_recv, part_send_sem, part_recv_sem),
                (sq_buf, sq_recv, sq_send_sem, sq_recv_sem),
            ):
                pltpu.make_async_remote_copy(
                    src_ref=src.at[layer, s],
                    dst_ref=dst.at[layer, s],
                    send_sem=ssem.at[layer, s],
                    recv_sem=rsem.at[layer, s],
                    device_id={"dp": s},
                    device_id_type=MESH,
                ).wait_recv()
            total = total + part_recv[layer, s].astype(F32)
            sq = sq + sq_recv[layer, s]
        mean = jnp.sum(
            jnp.where(row_lane == row_sub, sq[0:1, :], 0.0), axis=1, keepdims=True
        ) / features
        scale = lax.rsqrt(mean + NORM_EPS)
        total = total * scale
        u = total[:, :chans].astype(BF16)
        gate = total[:, chans:].astype(BF16).astype(F32)
        u_f = u.astype(F32)
        read = base[layer] + jnp.dot(
            jnp.concatenate([u, u], axis=1), mix_cat[layer], preferred_element_type=F32
        )
        y = jax.nn.gelu(read + feed[layer : layer + 1, :] * u_f)
        z_buf[layer, i] = (y * jax.nn.sigmoid(gate)).astype(BF16)
        for step in reversed(dp_steps):
            s = dp_peer(step)
            pltpu.make_async_remote_copy(
                src_ref=z_buf.at[layer, i],
                dst_ref=z_buf.at[layer, i],
                send_sem=z_send_sem.at[layer, s],
                recv_sem=z_recv_sem.at[layer, i],
                device_id={"dp": s},
                device_id_type=MESH,
            ).start()

        for step in [(0, 0), *dp_steps]:
            s = dp_peer(step)
            if step != (0, 0):
                pltpu.make_async_remote_copy(
                    src_ref=z_buf.at[layer, s],
                    dst_ref=z_buf.at[layer, s],
                    send_sem=z_send_sem.at[layer, s],
                    recv_sem=z_recv_sem.at[layer, s],
                    device_id={"dp": s},
                    device_id_type=MESH,
                ).wait_recv()
            terms = jnp.dot(z_buf[layer, s], w_out[layer], preferred_element_type=F32)
            for k in range(per_block):
                owner = s * per_block + k
                term_buf[layer, owner] = terms[k * chunk : (k + 1) * chunk].astype(BF16)
            for k in range(per_block):
                owner = s * per_block + k
                o = lax.rem(j - owner + n_tp, n_tp)
                past = lax.div(o, far + 1)
                reach = o + past * (n_tp - 2 * o)
                pl.when((lax.rem(reach, 3) != 0) & (reach != far))(
                    functools.partial(climb, layer, owner, o, past, reach)
                )
                pl.when(reach == far)(lambda: up(layer, far).start())

        spread = jnp.where(own_group[None], u_f[:, None, :], 0.0).astype(BF16)
        spread = spread.reshape(mine * groups, chans)
        driven = jnp.dot(spread, drive_high[layer], preferred_element_type=F32) + jnp.dot(
            spread, drive_low[layer], preferred_element_type=F32
        )
        state_out[layer] = carried[layer] + driven.reshape(mine, groups, width)

        if layer == 0:
            pl.semaphore_wait(relay, 2)
        else:
            await_sends(layer - 1)
        arrived(layer, far).wait_recv()
        for o in hubs:
            owner = at_offset(-o)
            total = term_buf[layer, owner].astype(F32)
            for c in children[o]:
                arrived(layer, c).wait_recv()
                total = total + term_recv[layer, c % n_tp].astype(F32)
            if abs(o) == hub:
                last = term_recv[layer, far].astype(F32)
                total = total + jnp.where(side * o > 0, last, 0.0)
            term_buf[layer, owner] = total.astype(BF16)
            up(layer, o).start()
        total = term_buf[layer, j].astype(F32)
        for o in sorted(children[0], key=abs):
            arrived(layer, o).wait_recv()
            total = total + term_recv[layer, o % n_tp].astype(F32)
        at = chunk_rows(j)
        branch = total.astype(BF16).astype(F32)
        x_buf[layer + 1, at, :] = (x_buf[layer, at, :].astype(F32) + branch).astype(BF16)

        for c in sorted(children[0], key=lambda o: -abs(o)):
            down(layer, 0, c).start()
        for o in sorted(hubs, key=abs):
            landed(layer, o).wait_recv()
            for c in sorted(children[o], key=lambda c: -abs(c)):
                down(layer, o, c).start()
        down(layer, hub * side, far * side).start()

        if layer + 1 < layers:
            order = [0]
            for d in range(1, n_dp // 2 + 1):
                order.append(d)
                if n_dp - d != d:
                    order.append(n_dp - d)
            for d in order:
                s = lax.rem(lax.div(j, per_block) + d, n_dp)
                for k in range(per_block):
                    t = s * per_block + k
                    o = lax.rem(j - t + n_tp, n_tp)
                    ready = o != 0
                    for h in hubs:
                        ready = ready & (o != h % n_tp)
                    pl.when(ready)(lambda o=o: landed(layer, o).wait_recv())
                piece = pl.ds(pl.multiple_of(s * mine, mine), mine)
                x = x_buf[layer + 1, piece, :].astype(F32)
                scaled = (x * norm[layer + 1 : layer + 2, :]).astype(BF16)
                sq_buf[layer + 1, s, :, pl.ds(0, mine)] = square_rows(x)[0:1]
                part_buf[layer + 1, s] = jnp.dot(
                    scaled, w_cat[layer + 1], preferred_element_type=F32
                ).astype(BF16)
                pl.when(s != i)(functools.partial(send_part, layer + 1, s))
        else:
            for o in [*leaves, far]:
                landed(layer, o).wait_recv()
            tokens_out[...] = x_buf[layers]

    await_sends(layers - 1)


def on_device(
    n_dp,
    n_tp,
    tokens,
    sequence_lengths,
    recurrent_state,
    norm_weight,
    input_weight,
    gate_weight,
    output_weight,
    negated_real_rate,
    frequency,
    discrete_step,
    group_input_matrix,
    group_output_matrix,
    feedthrough_weight,
    extra_log_decay,
):
    layers, mine, groups, width = recurrent_state.shape
    rows, local_d = tokens.shape
    chans = output_weight.shape[1]
    chunk = rows // n_tp
    hbm = pl.BlockSpec(memory_space=pltpu.HBM)
    dma = pltpu.SemaphoreType.DMA
    in_hbm = lambda a: pltpu.with_memory_space_constraint(a, pltpu.HBM)
    like = lambda a: pltpu.VMEM(a.shape, a.dtype)
    scratch = [
        pltpu.SMEM(sequence_lengths.shape, sequence_lengths.dtype),
        pltpu.SMEM(discrete_step.shape, discrete_step.dtype),
        pltpu.VMEM((layers + 1, rows, local_d), BF16),
        like(norm_weight),
        pltpu.VMEM((layers, local_d, 2 * chans), BF16),
        like(output_weight),
        like(extra_log_decay),
        like(recurrent_state),
        like(negated_real_rate),
        like(frequency),
        like(group_input_matrix),
        like(group_output_matrix),
        like(feedthrough_weight),
        dma((14,)),
        dma((layers + 1,)),
        pltpu.VMEM((layers, n_dp, mine, 2 * chans), BF16),
        pltpu.VMEM((layers, n_dp, mine, 2 * chans), BF16),
        dma((layers, n_dp)),
        dma((layers, n_dp)),
        pltpu.VMEM((layers, n_dp, 1, 128), F32),
        pltpu.VMEM((layers, n_dp, 1, 128), F32),
        dma((layers, n_dp)),
        dma((layers, n_dp)),
        pltpu.VMEM((layers, n_dp, mine, chans), BF16),
        dma((layers, n_dp)),
        dma((layers, n_dp)),
        pltpu.VMEM((layers, n_tp, chunk, local_d), BF16),
        pltpu.VMEM((layers, n_tp, chunk, local_d), BF16),
        dma((layers, n_tp)),
        dma((layers, n_tp)),
        dma((layers, n_tp)),
        dma((layers, n_tp)),
        pltpu.VMEM((mine, groups, width), F32),
        pltpu.VMEM((layers, mine, groups, width), F32),
        pltpu.VMEM((layers, chans, width), BF16),
        pltpu.VMEM((layers, chans, width), BF16),
        pltpu.VMEM((layers, 2 * chans, chans), BF16),
        pltpu.VMEM((layers, mine, chans), F32),
        pltpu.SemaphoreType.REGULAR,
    ]
    return pl.pallas_call(
        functools.partial(kernel, n_dp, n_tp, n_dp * local_d),
        out_shape=(
            jax.ShapeDtypeStruct(tokens.shape, tokens.dtype),
            jax.ShapeDtypeStruct(recurrent_state.shape, recurrent_state.dtype),
        ),
        in_specs=[hbm] * 14,
        out_specs=(pl.BlockSpec(memory_space=pltpu.VMEM),) * 2,
        scratch_shapes=scratch,
        compiler_params=pltpu.CompilerParams(collective_id=0, has_side_effects=True, vmem_limit_bytes=16 * 2**20),
    )(
        in_hbm(sequence_lengths),
        in_hbm(discrete_step),
        in_hbm(tokens),
        in_hbm(norm_weight),
        in_hbm(input_weight),
        in_hbm(gate_weight),
        in_hbm(extra_log_decay),
        in_hbm(recurrent_state),
        in_hbm(negated_real_rate),
        in_hbm(frequency),
        in_hbm(group_input_matrix),
        in_hbm(group_output_matrix),
        in_hbm(feedthrough_weight),
        in_hbm(output_weight),
    )


def solution(mesh):
    in_specs = (
        P("grp", "dp"),
        P(("grp", "dp")),
        P(None, ("grp", "dp"), "tp", None),
        P(None, "dp"),
        P(None, "dp", "tp"),
        P(None, "dp", "tp"),
        P(None, "tp", "dp"),
        P(None, "tp"),
        P(None, "tp"),
        P(None, "tp"),
        P(None, "tp", None, None),
        P(None, "tp", None, None),
        P(None, "tp"),
        P(None, "tp", None),
    )
    out_specs = (P("grp", "dp"), P(None, ("grp", "dp"), "tp", None))
    return jax.shard_map(
        functools.partial(on_device, mesh.shape["dp"], mesh.shape["tp"]),
        mesh=mesh,
        in_specs=in_specs,
        out_specs=out_specs,
        check_vma=False,
    )
```

```python
import functools

import jax
import jax.numpy as jnp
from jax import lax
from jax.experimental import pallas as pl
from jax.experimental.pallas import tpu as pltpu
from jax.sharding import PartitionSpec as P

NORM_EPS = 1e-06
HIGHEST = lax.Precision.HIGHEST
F32 = jnp.float32
BF16 = jnp.bfloat16
MESH = pl.DeviceIdType.MESH


def contract_last(a, b, precision=None):
    return lax.dot_general(
        a, b, (((1,), (1,)), ((), ())), precision=precision, preferred_element_type=F32
    )


def split_two(a):
    high = a.astype(BF16)
    return high, (a - high.astype(F32)).astype(BF16)


def exp_less_one(x, exp_x):
    series = jnp.full_like(x, 1.0 / 3628800.0)
    for factor in (362880.0, 40320.0, 5040.0, 720.0, 120.0, 24.0, 6.0, 2.0, 1.0):
        series = series * x + 1.0 / factor
    return jnp.where(jnp.abs(x) < 0.6, series * x, exp_x - 1.0)


def sign(o):
    return 1 if o > 0 else -1


def step_to_hub(o):
    near = (abs(o) + 1) // 3 * 3
    return abs(o) if near in (0, abs(o)) else abs(o) - near


def kernel(
    n_dp,
    n_tp,
    features,
    lengths_hbm,
    step_hbm,
    tokens_hbm,
    norm_hbm,
    w_in_hbm,
    w_gate_hbm,
    decay_hbm,
    state_hbm,
    rate_hbm,
    freq_hbm,
    b_hbm,
    c_hbm,
    feed_hbm,
    w_out_hbm,
    tokens_out,
    state_out,
    lengths,
    step_width,
    x_buf,
    norm,
    w_cat,
    w_out,
    decay,
    state,
    rate,
    freq,
    b_mat,
    c_mat,
    feed,
    local_sem,
    part_buf,
    part_recv,
    part_send_sem,
    part_recv_sem,
    sq_buf,
    sq_recv,
    sq_send_sem,
    sq_recv_sem,
    z_buf,
    z_send_sem,
    z_recv_sem,
    term_buf,
    term_recv,
    term_send_sem,
    term_recv_sem,
    x_send_sem,
    x_recv_sem,
    pick,
    carried,
    drive_high,
    drive_low,
    mix_cat,
    base,
    relay,
):
    i = lax.axis_index("dp")
    j = lax.axis_index("tp")
    layers, mine, groups, width = state.shape
    half = width // 2
    rows, local_d = x_buf.shape[1:]
    chans = w_out.shape[1]
    chunk = rows // n_tp
    per_block = mine // chunk
    channel_group = chans // groups

    dp_steps = [(0, 1)] + [
        (d, e) for d in (1, n_dp // 2 - 1, n_dp // 4) for e in (0, 1)
    ]

    def dp_peer(step):
        d, e = step
        return lax.rem(lax.div(i, 2) + d, n_dp // 2) * 2 + lax.rem(lax.rem(i, 2) + e, 2)

    side = 1 - 2 * lax.rem(j, 2)
    far = n_tp // 2
    hub = far - 2
    tree = {o: o - sign(o) * step_to_hub(o) for o in range(1 - far, far) if o}
    children = {p: [o for o in tree if tree[o] == p] for p in [0, *tree]}
    by_reach = sorted(tree, key=lambda o: (-abs(o), o))
    leaves = [o for o in by_reach if not children[o]]
    hubs = [o for o in by_reach if children[o]]

    def at_offset(o):
        return lax.rem(j + o + n_tp, n_tp)

    loads = {}
    for n, (name, src, dst) in enumerate(
        [
            ("x", tokens_hbm, x_buf.at[0]),
            ("norm", norm_hbm, norm),
            ("w_in", w_in_hbm, w_cat.at[:, :, pl.ds(0, chans)]),
            ("w_gate", w_gate_hbm, w_cat.at[:, :, pl.ds(chans, chans)]),
            ("decay", decay_hbm, decay),
            ("state", state_hbm, state),
            ("rate", rate_hbm, rate),
            ("freq", freq_hbm, freq),
            ("b", b_hbm, b_mat),
            ("c", c_hbm, c_mat),
            ("feed", feed_hbm, feed),
            ("lengths", lengths_hbm, lengths),
            ("step", step_hbm, step_width),
            ("w_out", w_out_hbm, w_out),
        ]
    ):
        loads[name] = pltpu.make_async_copy(src, dst, local_sem.at[n])
    for name in ("x", "norm", "w_in", "w_gate"):
        loads[name].start()

    barrier = pltpu.get_barrier_semaphore()
    for step in dp_steps:
        pl.semaphore_signal(barrier, inc=1, device_id={"dp": dp_peer(step)}, device_id_type=MESH)
    tp_greeted = [o for o in (-3, 3, -2, 2, -1, 1)]
    for step in tp_greeted:
        pl.semaphore_signal(barrier, inc=1, device_id={"tp": at_offset(step)}, device_id_type=MESH)

    later = [name for name in loads if name not in ("x", "norm", "w_in", "w_gate")]
    for name in later:
        loads[name].start()

    lane = lax.broadcasted_iota(jnp.int32, (groups, width), 1)
    sub = lax.broadcasted_iota(jnp.int32, (groups, width), 0)
    low = lane < half
    col_group = lax.broadcasted_iota(jnp.int32, (groups, chans), 1) // channel_group
    own_group = col_group == lax.broadcasted_iota(jnp.int32, (groups, chans), 0)
    block_row = lax.broadcasted_iota(jnp.int32, (chans, chans), 0) // channel_group
    block_col = lax.broadcasted_iota(jnp.int32, (chans, chans), 1) // channel_group

    def by_group(ref, layer):
        out = jnp.zeros((groups, width), F32)
        for g in range(groups):
            pair = ref[layer : layer + 1, (g // 2) * width : (g // 2 + 1) * width]
            other = pltpu.roll(pair, half, 1)
            row = jnp.where(low[:1] if g % 2 == 0 else ~low[:1], pair, other)
            out = jnp.where(sub == g, row, out)
        return out

    def prepare(layer):
        dt = jnp.zeros((groups, width), F32)
        for g in range(groups):
            dt = jnp.where(sub == g, step_width[layer, g], dt)
        a_re = by_group(rate, layer)
        a_im = by_group(freq, layer)
        log_mag = -a_re * dt
        turn = a_im * dt
        magnitude = jnp.exp(log_mag)
        cosine = jnp.cos(turn)
        disc_re = magnitude * cosine
        disc_im = magnitude * jnp.sin(turn)
        half_sine = jnp.sin(0.5 * turn)
        numer_re = exp_less_one(log_mag, magnitude) * cosine - 2.0 * half_sine * half_sine
        denom = a_re * a_re + a_im * a_im
        drive_re = (-numer_re * a_re + disc_im * a_im) / denom
        drive_im = (-disc_im * a_re - numer_re * a_im) / denom
        disc_cross = jnp.where(low, -disc_im, disc_im)
        drive_cross = jnp.where(low, -drive_im, drive_im)

        b_l = b_mat[layer]
        drive = drive_re[:, None, :] * b_l + drive_cross[:, None, :] * pltpu.roll(b_l, half, 2)
        drive = drive.reshape(chans, width)
        high, rest = split_two(drive)
        drive_high[layer] = high
        drive_low[layer] = rest
        c_l = jnp.where(low[:1][None], c_mat[layer], -c_mat[layer]).reshape(chans, width)
        mix = jnp.where(block_row == block_col, contract_last(drive, c_l, HIGHEST), 0.0)
        high, rest = split_two(mix)
        mix_cat[layer, :chans] = high
        mix_cat[layer, chans:] = rest

        for r in range(mine):
            offset = lane - (lengths[r] - 1)
            found = jnp.zeros((groups, width), F32)
            for at in range(0, decay.shape[2], width):
                found = jnp.where(offset == -at, decay[layer, :, at : at + width], found)
            pick[r] = found
        extra = jnp.exp(jnp.sum(pick[...], axis=-1, keepdims=True))
        s = state[layer]
        kept = extra * (disc_re[None] * s + disc_cross[None] * pltpu.roll(s, half, 2))
        carried[layer] = kept
        read = contract_last(kept.reshape(mine * groups, width), c_l, HIGHEST)
        read = jnp.where(own_group[None], read.reshape(mine, groups, chans), 0.0)
        base[layer] = jnp.sum(read, axis=1)

    def send_part(layer, s):
        for src, dst, ssem, rsem in (
            (part_buf, part_recv, part_send_sem, part_recv_sem),
            (sq_buf, sq_recv, sq_send_sem, sq_recv_sem),
        ):
            pltpu.make_async_remote_copy(
                src_ref=src.at[layer, s],
                dst_ref=dst.at[layer, i],
                send_sem=ssem.at[0],
                recv_sem=rsem.at[0],
                device_id={"dp": s},
                device_id_type=MESH,
            ).start()

    def await_sends():
        for buf, sem in (
            (part_buf.at[:, pl.ds(0, n_dp - 1)], part_send_sem),
            (sq_buf.at[:, pl.ds(0, n_dp - 1)], sq_send_sem),
            (z_buf.at[:, pl.ds(0, n_dp - 1)], z_send_sem),
            (term_buf.at[:, pl.ds(0, n_tp - 1)], term_send_sem),
            (x_buf.at[pl.ds(0, layers), pl.ds(0, rows - chunk)], x_send_sem),
        ):
            pltpu.make_async_copy(buf, buf, sem.at[0]).wait()

    ones = jnp.ones((8, 128), F32)

    def square_rows(x):
        x2 = x * x
        total = x2[:, 0:128]
        for k in range(1, local_d // 128):
            total = total + x2[:, k * 128 : (k + 1) * 128]
        return contract_last(ones, total, HIGHEST)

    def chunk_rows(t):
        return pl.ds(pl.multiple_of(t * chunk, chunk), chunk)

    def up(layer, o):
        hop = 2 * side if o == far else o - tree[o]
        owner = at_offset(-o)
        return pltpu.make_async_remote_copy(
            src_ref=term_buf.at[layer, owner],
            dst_ref=term_recv.at[layer, o % n_tp],
            send_sem=term_send_sem.at[0],
            recv_sem=term_recv_sem.at[o % n_tp],
            device_id={"tp": at_offset(-hop)},
            device_id_type=MESH,
        )

    arrived = up

    def climb(layer, owner, o, past, reach):
        hop = (1 - 2 * past) * (reach - lax.div(reach + 1, 3) * 3)
        pltpu.make_async_remote_copy(
            src_ref=term_buf.at[layer, owner],
            dst_ref=term_recv.at[layer, o],
            send_sem=term_send_sem.at[0],
            recv_sem=term_recv_sem.at[o],
            device_id={"tp": at_offset(-hop)},
            device_id_type=MESH,
        ).start()

    def down(layer, o, c):
        owner = chunk_rows(at_offset(-o))
        slot = lax.rem(c + n_tp, n_tp)
        return pltpu.make_async_remote_copy(
            src_ref=x_buf.at[layer + 1, owner],
            dst_ref=x_buf.at[layer + 1, owner],
            send_sem=x_send_sem.at[0],
            recv_sem=x_recv_sem.at[slot],
            device_id={"tp": at_offset(c - o)},
            device_id_type=MESH,
        )

    def landed(layer, o):
        owner = chunk_rows(at_offset(-o))
        slot = lax.rem(o + n_tp, n_tp)
        return pltpu.make_async_remote_copy(
            src_ref=x_buf.at[layer + 1, owner],
            dst_ref=x_buf.at[layer + 1, owner],
            send_sem=x_send_sem.at[0],
            recv_sem=x_recv_sem.at[slot],
            device_id={"tp": at_offset(1)},
            device_id_type=MESH,
        )


    loads["x"].wait()
    loads["norm"].wait()
    x = x_buf[0].astype(F32)
    scaled = (x * norm[0:1, :]).astype(BF16)
    squares = square_rows(x)
    for s in range(n_dp):
        sq_buf[0, s, :, pl.ds(0, mine)] = squares[0:1, s * mine : (s + 1) * mine]
    loads["w_in"].wait()
    loads["w_gate"].wait()
    part_buf[0] = (
        jnp.dot(scaled, w_cat[0], preferred_element_type=F32)
        .astype(BF16)
        .reshape(n_dp, mine, 2 * chans)
    )
    pl.semaphore_wait(barrier, len(dp_steps) + len(tp_greeted))
    for step in (-hub // 2, hub // 2):
        pl.semaphore_signal(relay, inc=1, device_id={"tp": at_offset(step)}, device_id_type=MESH)
    for step in reversed(dp_steps):
        send_part(0, dp_peer(step))
    for name in later:
        loads[name].wait()
    for layer in range(layers):
        prepare(layer)

    row_lane = lax.broadcasted_iota(jnp.int32, (mine, 128), 1)
    row_sub = lax.broadcasted_iota(jnp.int32, (mine, 128), 0)

    for layer in range(layers):
        for buf, sem in ((part_recv, part_recv_sem), (sq_recv, sq_recv_sem)):
            others = buf.at[layer, pl.ds(0, n_dp - 1)]
            pltpu.make_async_copy(others, others, sem.at[0]).wait()
        total = part_buf[layer, i].astype(F32)
        sq = sq_buf[layer, i]
        for step in dp_steps:
            s = dp_peer(step)
            total = total + part_recv[layer, s].astype(F32)
            sq = sq + sq_recv[layer, s]
        mean = jnp.sum(
            jnp.where(row_lane == row_sub, sq[0:1, :], 0.0), axis=1, keepdims=True
        ) / features
        scale = lax.rsqrt(mean + NORM_EPS)
        total = total * scale
        u = total[:, :chans].astype(BF16)
        gate = total[:, chans:].astype(BF16).astype(F32)
        u_f = u.astype(F32)
        read = base[layer] + jnp.dot(
            jnp.concatenate([u, u], axis=1), mix_cat[layer], preferred_element_type=F32
        )
        y = jax.nn.gelu(read + feed[layer : layer + 1, :] * u_f)
        z_buf[layer, i] = (y * jax.nn.sigmoid(gate)).astype(BF16)
        for step in reversed(dp_steps):
            s = dp_peer(step)
            pltpu.make_async_remote_copy(
                src_ref=z_buf.at[layer, i],
                dst_ref=z_buf.at[layer, i],
                send_sem=z_send_sem.at[0],
                recv_sem=z_recv_sem.at[i],
                device_id={"dp": s},
                device_id_type=MESH,
            ).start()

        for step in [(0, 0), *dp_steps]:
            s = dp_peer(step)
            if step != (0, 0):
                pltpu.make_async_remote_copy(
                    src_ref=z_buf.at[layer, s],
                    dst_ref=z_buf.at[layer, s],
                    send_sem=z_send_sem.at[0],
                    recv_sem=z_recv_sem.at[s],
                    device_id={"dp": s},
                    device_id_type=MESH,
                ).wait_recv()
            terms = jnp.dot(z_buf[layer, s], w_out[layer], preferred_element_type=F32)
            for k in range(per_block):
                owner = s * per_block + k
                term_buf[layer, owner] = terms[k * chunk : (k + 1) * chunk].astype(BF16)
            for k in range(per_block):
                owner = s * per_block + k
                o = lax.rem(j - owner + n_tp, n_tp)
                past = lax.div(o, far + 1)
                reach = o + past * (n_tp - 2 * o)
                pl.when((lax.rem(reach, 3) != 0) & (reach != far))(
                    functools.partial(climb, layer, owner, o, past, reach)
                )
                pl.when(reach == far)(lambda: up(layer, far).start())

        spread = jnp.where(own_group[None], u_f[:, None, :], 0.0).astype(BF16)
        spread = spread.reshape(mine * groups, chans)
        driven = jnp.dot(spread, drive_high[layer], preferred_element_type=F32) + jnp.dot(
            spread, drive_low[layer], preferred_element_type=F32
        )
        state_out[layer] = carried[layer] + driven.reshape(mine, groups, width)

        if layer == 0:
            pl.semaphore_wait(relay, 2)
        arrived(layer, far).wait_recv()
        for o in hubs:
            owner = at_offset(-o)
            total = term_buf[layer, owner].astype(F32)
            for c in children[o]:
                arrived(layer, c).wait_recv()
                total = total + term_recv[layer, c % n_tp].astype(F32)
            if abs(o) == hub:
                last = term_recv[layer, far].astype(F32)
                total = total + jnp.where(side * o > 0, last, 0.0)
            term_buf[layer, owner] = total.astype(BF16)
            up(layer, o).start()
        total = term_buf[layer, j].astype(F32)
        for o in sorted(children[0], key=abs):
            arrived(layer, o).wait_recv()
            total = total + term_recv[layer, o % n_tp].astype(F32)
        at = chunk_rows(j)
        branch = total.astype(BF16).astype(F32)
        x_buf[layer + 1, at, :] = (x_buf[layer, at, :].astype(F32) + branch).astype(BF16)

        for c in sorted(children[0], key=lambda o: -abs(o)):
            down(layer, 0, c).start()
        for o in sorted(hubs, key=abs):
            landed(layer, o).wait_recv()
            for c in sorted(children[o], key=lambda c: -abs(c)):
                down(layer, o, c).start()
        down(layer, hub * side, far * side).start()

        if layer + 1 < layers:
            order = [0]
            for d in range(1, n_dp // 2 + 1):
                order.append(d)
                if n_dp - d != d:
                    order.append(n_dp - d)
            for d in order:
                s = lax.rem(lax.div(j, per_block) + d, n_dp)
                for k in range(per_block):
                    t = s * per_block + k
                    o = lax.rem(j - t + n_tp, n_tp)
                    ready = o != 0
                    for h in hubs:
                        ready = ready & (o != h % n_tp)
                    pl.when(ready)(lambda o=o: landed(layer, o).wait_recv())
                piece = pl.ds(pl.multiple_of(s * mine, mine), mine)
                x = x_buf[layer + 1, piece, :].astype(F32)
                scaled = (x * norm[layer + 1 : layer + 2, :]).astype(BF16)
                sq_buf[layer + 1, s, :, pl.ds(0, mine)] = square_rows(x)[0:1]
                part_buf[layer + 1, s] = jnp.dot(
                    scaled, w_cat[layer + 1], preferred_element_type=F32
                ).astype(BF16)
                pl.when(s != i)(functools.partial(send_part, layer + 1, s))
        else:
            for o in [*leaves, far]:
                landed(layer, o).wait_recv()
            tokens_out[...] = x_buf[layers]

    await_sends()


def on_device(
    n_dp,
    n_tp,
    tokens,
    sequence_lengths,
    recurrent_state,
    norm_weight,
    input_weight,
    gate_weight,
    output_weight,
    negated_real_rate,
    frequency,
    discrete_step,
    group_input_matrix,
    group_output_matrix,
    feedthrough_weight,
    extra_log_decay,
):
    layers, mine, groups, width = recurrent_state.shape
    rows, local_d = tokens.shape
    chans = output_weight.shape[1]
    chunk = rows // n_tp
    hbm = pl.BlockSpec(memory_space=pltpu.HBM)
    dma = pltpu.SemaphoreType.DMA
    in_hbm = lambda a: pltpu.with_memory_space_constraint(a, pltpu.HBM)
    like = lambda a: pltpu.VMEM(a.shape, a.dtype)
    scratch = [
        pltpu.SMEM(sequence_lengths.shape, sequence_lengths.dtype),
        pltpu.SMEM(discrete_step.shape, discrete_step.dtype),
        pltpu.VMEM((layers + 1, rows, local_d), BF16),
        like(norm_weight),
        pltpu.VMEM((layers, local_d, 2 * chans), BF16),
        like(output_weight),
        like(extra_log_decay),
        like(recurrent_state),
        like(negated_real_rate),
        like(frequency),
        like(group_input_matrix),
        like(group_output_matrix),
        like(feedthrough_weight),
        dma((14,)),
        pltpu.VMEM((layers, n_dp, mine, 2 * chans), BF16),
        pltpu.VMEM((layers, n_dp, mine, 2 * chans), BF16),
        dma((1,)),
        dma((1,)),
        pltpu.VMEM((layers, n_dp, 1, 128), F32),
        pltpu.VMEM((layers, n_dp, 1, 128), F32),
        dma((1,)),
        dma((1,)),
        pltpu.VMEM((layers, n_dp, mine, chans), BF16),
        dma((1,)),
        dma((n_dp,)),
        pltpu.VMEM((layers, n_tp, chunk, local_d), BF16),
        pltpu.VMEM((layers, n_tp, chunk, local_d), BF16),
        dma((1,)),
        dma((n_tp,)),
        dma((1,)),
        dma((n_tp,)),
        pltpu.VMEM((mine, groups, width), F32),
        pltpu.VMEM((layers, mine, groups, width), F32),
        pltpu.VMEM((layers, chans, width), BF16),
        pltpu.VMEM((layers, chans, width), BF16),
        pltpu.VMEM((layers, 2 * chans, chans), BF16),
        pltpu.VMEM((layers, mine, chans), F32),
        pltpu.SemaphoreType.REGULAR,
    ]
    return pl.pallas_call(
        functools.partial(kernel, n_dp, n_tp, n_dp * local_d),
        out_shape=(
            jax.ShapeDtypeStruct(tokens.shape, tokens.dtype),
            jax.ShapeDtypeStruct(recurrent_state.shape, recurrent_state.dtype),
        ),
        in_specs=[hbm] * 14,
        out_specs=(pl.BlockSpec(memory_space=pltpu.VMEM),) * 2,
        scratch_shapes=scratch,
        compiler_params=pltpu.CompilerParams(collective_id=0, has_side_effects=True, vmem_limit_bytes=16 * 2**20),
    )(
        in_hbm(sequence_lengths),
        in_hbm(discrete_step),
        in_hbm(tokens),
        in_hbm(norm_weight),
        in_hbm(input_weight),
        in_hbm(gate_weight),
        in_hbm(extra_log_decay),
        in_hbm(recurrent_state),
        in_hbm(negated_real_rate),
        in_hbm(frequency),
        in_hbm(group_input_matrix),
        in_hbm(group_output_matrix),
        in_hbm(feedthrough_weight),
        in_hbm(output_weight),
    )


def solution(mesh):
    in_specs = (
        P("grp", "dp"),
        P(("grp", "dp")),
        P(None, ("grp", "dp"), "tp", None),
        P(None, "dp"),
        P(None, "dp", "tp"),
        P(None, "dp", "tp"),
        P(None, "tp", "dp"),
        P(None, "tp"),
        P(None, "tp"),
        P(None, "tp"),
        P(None, "tp", None, None),
        P(None, "tp", None, None),
        P(None, "tp"),
        P(None, "tp", None),
    )
    out_specs = (P("grp", "dp"), P(None, ("grp", "dp"), "tp", None))
    return jax.shard_map(
        functools.partial(on_device, mesh.shape["dp"], mesh.shape["tp"]),
        mesh=mesh,
        in_specs=in_specs,
        out_specs=out_specs,
        check_vma=False,
    )
```

```python
import functools

import jax
import jax.numpy as jnp
from jax import lax
from jax.experimental import pallas as pl
from jax.experimental.pallas import tpu as pltpu
from jax.sharding import PartitionSpec as P

NORM_EPS = 1e-06
HIGHEST = lax.Precision.HIGHEST
F32 = jnp.float32
BF16 = jnp.bfloat16
MESH = pl.DeviceIdType.MESH


def contract_last(a, b, precision=None):
    return lax.dot_general(
        a, b, (((1,), (1,)), ((), ())), precision=precision, preferred_element_type=F32
    )


def split_two(a):
    high = a.astype(BF16)
    return high, (a - high.astype(F32)).astype(BF16)


def exp_less_one(x, exp_x):
    series = jnp.full_like(x, 1.0 / 3628800.0)
    for factor in (362880.0, 40320.0, 5040.0, 720.0, 120.0, 24.0, 6.0, 2.0, 1.0):
        series = series * x + 1.0 / factor
    return jnp.where(jnp.abs(x) < 0.6, series * x, exp_x - 1.0)


def sign(o):
    return 1 if o > 0 else -1


def step_to_hub(o):
    near = (abs(o) + 1) // 3 * 3
    return abs(o) if near in (0, abs(o)) else abs(o) - near


def kernel(
    n_dp,
    n_tp,
    features,
    lengths_hbm,
    step_hbm,
    tokens_hbm,
    norm_hbm,
    w_in_hbm,
    w_gate_hbm,
    decay_hbm,
    state_hbm,
    rate_hbm,
    freq_hbm,
    b_hbm,
    c_hbm,
    feed_hbm,
    w_out_hbm,
    tokens_out,
    state_out,
    lengths,
    step_width,
    x_buf,
    norm,
    w_cat,
    w_out,
    decay,
    state,
    rate,
    freq,
    b_mat,
    c_mat,
    feed,
    local_sem,
    part_buf,
    part_recv,
    part_send_sem,
    part_recv_sem,
    sq_buf,
    sq_recv,
    sq_send_sem,
    sq_recv_sem,
    z_buf,
    z_send_sem,
    z_recv_sem,
    term_buf,
    term_recv,
    term_send_sem,
    term_recv_sem,
    x_send_sem,
    x_recv_sem,
    pick,
    carried,
    drive_high,
    drive_low,
    mix_cat,
    base,
    relay,
):
    i = lax.axis_index("dp")
    j = lax.axis_index("tp")
    layers, mine, groups, width = state.shape
    half = width // 2
    halves, per_block, chunk, local_d = x_buf.shape[2:]
    rows = n_dp * mine
    part_rows = mine // halves
    chans = w_out.shape[1]
    channel_group = chans // groups

    dp_steps = [(0, 1)] + [
        (d, e) for d in (1, n_dp // 2 - 1, n_dp // 4) for e in (0, 1)
    ]

    def dp_peer(step):
        d, e = step
        return lax.rem(lax.div(i, 2) + d, n_dp // 2) * 2 + lax.rem(lax.rem(i, 2) + e, 2)

    side = 1 - 2 * lax.rem(j, 2)
    far = n_tp // 2
    hub = far - 2
    tree = {o: o - sign(o) * step_to_hub(o) for o in range(1 - far, far) if o}
    children = {p: [o for o in tree if tree[o] == p] for p in [0, *tree]}
    by_reach = sorted(tree, key=lambda o: (-abs(o), o))
    leaves = [o for o in by_reach if not children[o]]
    hubs = [o for o in by_reach if children[o]]

    near_hub = [c for o in hubs if abs(o) != hub for c in children[o]]
    far_hub = [c for o in hubs if abs(o) == hub for c in children[o]] + [far]
    up_group = {o: 0 if o in far_hub else 1 if o in near_hub else 2 for o in [*tree, far]}
    down_group = {o: 1 + hubs.index(o) if o in hubs else 0 for o in [*tree, far]}

    def at_offset(o):
        return lax.rem(j + o + n_tp, n_tp)

    loads = {}
    for n, (name, src, dst) in enumerate(
        [
            ("x", tokens_hbm, x_buf.at[0]),
            ("norm", norm_hbm, norm),
            ("w_in", w_in_hbm.at[0], w_cat.at[0, :, pl.ds(0, chans)]),
            ("w_gate", w_gate_hbm.at[0], w_cat.at[0, :, pl.ds(chans, chans)]),
            ("w_in_1", w_in_hbm.at[1], w_cat.at[1, :, pl.ds(0, chans)]),
            ("w_gate_1", w_gate_hbm.at[1], w_cat.at[1, :, pl.ds(chans, chans)]),
            ("decay", decay_hbm, decay),
            ("state", state_hbm, state),
            ("rate", rate_hbm, rate),
            ("freq", freq_hbm, freq),
            ("b", b_hbm, b_mat),
            ("c", c_hbm, c_mat),
            ("feed", feed_hbm, feed),
            ("lengths", lengths_hbm, lengths),
            ("step", step_hbm, step_width),
            ("w_out", w_out_hbm, w_out),
        ]
    ):
        loads[name] = pltpu.make_async_copy(src, dst, local_sem.at[n])
    for name in ("x", "norm", "w_in", "w_gate"):
        loads[name].start()

    barrier = pltpu.get_barrier_semaphore()
    for step in dp_steps:
        pl.semaphore_signal(barrier, inc=1, device_id={"dp": dp_peer(step)}, device_id_type=MESH)
    tp_greeted = [o for o in (-3, 3, -2, 2, -1, 1)]
    for step in tp_greeted:
        pl.semaphore_signal(barrier, inc=1, device_id={"tp": at_offset(step)}, device_id_type=MESH)

    later = [name for name in loads if name not in ("x", "norm", "w_in", "w_gate")]
    for name in later:
        loads[name].start()

    lane = lax.broadcasted_iota(jnp.int32, (groups, width), 1)
    sub = lax.broadcasted_iota(jnp.int32, (groups, width), 0)
    low = lane < half
    col_group = lax.broadcasted_iota(jnp.int32, (groups, chans), 1) // channel_group
    own_group = col_group == lax.broadcasted_iota(jnp.int32, (groups, chans), 0)
    block_row = lax.broadcasted_iota(jnp.int32, (chans, chans), 0) // channel_group
    block_col = lax.broadcasted_iota(jnp.int32, (chans, chans), 1) // channel_group

    def by_group(ref, layer):
        out = jnp.zeros((groups, width), F32)
        for g in range(groups):
            pair = ref[layer : layer + 1, (g // 2) * width : (g // 2 + 1) * width]
            other = pltpu.roll(pair, half, 1)
            row = jnp.where(low[:1] if g % 2 == 0 else ~low[:1], pair, other)
            out = jnp.where(sub == g, row, out)
        return out

    def prepare(layer):
        dt = jnp.zeros((groups, width), F32)
        for g in range(groups):
            dt = jnp.where(sub == g, step_width[layer, g], dt)
        a_re = by_group(rate, layer)
        a_im = by_group(freq, layer)
        log_mag = -a_re * dt
        turn = a_im * dt
        magnitude = jnp.exp(log_mag)
        cosine = jnp.cos(turn)
        disc_re = magnitude * cosine
        disc_im = magnitude * jnp.sin(turn)
        half_sine = jnp.sin(0.5 * turn)
        numer_re = exp_less_one(log_mag, magnitude) * cosine - 2.0 * half_sine * half_sine
        denom = a_re * a_re + a_im * a_im
        drive_re = (-numer_re * a_re + disc_im * a_im) / denom
        drive_im = (-disc_im * a_re - numer_re * a_im) / denom
        disc_cross = jnp.where(low, -disc_im, disc_im)
        drive_cross = jnp.where(low, -drive_im, drive_im)

        b_l = b_mat[layer]
        drive = drive_re[:, None, :] * b_l + drive_cross[:, None, :] * pltpu.roll(b_l, half, 2)
        drive = drive.reshape(chans, width)
        high, rest = split_two(drive)
        drive_high[layer] = high
        drive_low[layer] = rest
        c_l = jnp.where(low[:1][None], c_mat[layer], -c_mat[layer]).reshape(chans, width)
        mix = jnp.where(block_row == block_col, contract_last(drive, c_l, HIGHEST), 0.0)
        high, rest = split_two(mix)
        mix_cat[layer, :chans] = high
        mix_cat[layer, chans:] = rest

        for r in range(mine):
            offset = lane - (lengths[r] - 1)
            found = jnp.zeros((groups, width), F32)
            for at in range(0, decay.shape[2], width):
                found = jnp.where(offset == -at, decay[layer, :, at : at + width], found)
            pick[r] = found
        extra = jnp.exp(jnp.sum(pick[...], axis=-1, keepdims=True))
        s = state[layer]
        kept = extra * (disc_re[None] * s + disc_cross[None] * pltpu.roll(s, half, 2))
        carried[layer] = kept
        read = contract_last(kept.reshape(mine * groups, width), c_l, HIGHEST)
        read = jnp.where(own_group[None], read.reshape(mine, groups, chans), 0.0)
        base[layer] = jnp.sum(read, axis=1)

    def send_part(layer, h, s):
        for src, dst, ssem, rsem in (
            (part_buf, part_recv, part_send_sem, part_recv_sem),
            (sq_buf, sq_recv, sq_send_sem, sq_recv_sem),
        ):
            pltpu.make_async_remote_copy(
                src_ref=src.at[layer, h, s],
                dst_ref=dst.at[layer, h, i],
                send_sem=ssem.at[0],
                recv_sem=rsem.at[h],
                device_id={"dp": s},
                device_id_type=MESH,
            ).start()

    def await_sends():
        for buf, sem in (
            (part_buf.at[:, :, pl.ds(0, n_dp - 1)], part_send_sem),
            (sq_buf.at[:, :, pl.ds(0, n_dp - 1)], sq_send_sem),
            (z_buf.at[:, :, pl.ds(0, n_dp - 1)], z_send_sem),
            (term_buf.at[:, :, pl.ds(0, n_tp - 1)], term_send_sem),
            (term_buf.at[:, :, pl.ds(0, n_tp - 1)], x_send_sem),
        ):
            pltpu.make_async_copy(buf, buf, sem.at[0]).wait()

    ones = jnp.ones((8, 128), F32)

    def square_rows(x):
        x2 = x * x
        total = x2[:, 0:128]
        for k in range(1, local_d // 128):
            total = total + x2[:, k * 128 : (k + 1) * 128]
        return contract_last(ones, total, HIGHEST)

    def of_owner(layer, h, t):
        return x_buf.at[layer, lax.div(t, per_block), h, lax.rem(t, per_block)]

    def up(layer, h, o):
        hop = 2 * side if o == far else o - tree[o]
        owner = at_offset(-o)
        return pltpu.make_async_remote_copy(
            src_ref=term_buf.at[layer, h, owner],
            dst_ref=term_recv.at[layer, h, o % n_tp],
            send_sem=term_send_sem.at[0],
            recv_sem=term_recv_sem.at[h, up_group[o]],
            device_id={"tp": at_offset(-hop)},
            device_id_type=MESH,
        )

    def climb(layer, h, owner, o, past, reach):
        hop = (1 - 2 * past) * (reach - lax.div(reach + 1, 3) * 3)
        pltpu.make_async_remote_copy(
            src_ref=term_buf.at[layer, h, owner],
            dst_ref=term_recv.at[layer, h, o],
            send_sem=term_send_sem.at[0],
            recv_sem=term_recv_sem.at[h, 2 - lax.div(reach + 1, 3)],
            device_id={"tp": at_offset(-hop)},
            device_id_type=MESH,
        ).start()

    def down(layer, h, o, c):
        piece = of_owner(layer + 1, h, at_offset(-o))
        return pltpu.make_async_remote_copy(
            src_ref=piece,
            dst_ref=piece,
            send_sem=x_send_sem.at[0],
            recv_sem=x_recv_sem.at[h, down_group.get(c if isinstance(c, int) else far, 0)],
            device_id={"tp": at_offset(c - o)},
            device_id_type=MESH,
        )

    def await_copies(buf, count, sem):
        some = buf.at[pl.ds(0, count)]
        pltpu.make_async_copy(some, some, sem).wait()

    def await_hub_chunk(layer, h, o):
        await_copies(term_buf.at[layer, h], 1, x_recv_sem.at[h, down_group[o]])

    def await_leaf_chunks(layer, h):
        await_copies(term_buf.at[layer, h], len(leaves) + 1, x_recv_sem.at[h, 0])

    def z_copy(layer, h, s, owner):
        return pltpu.make_async_remote_copy(
            src_ref=z_buf.at[layer, h, owner],
            dst_ref=z_buf.at[layer, h, owner],
            send_sem=z_send_sem.at[0],
            recv_sem=z_recv_sem.at[owner if h == 0 else n_dp],
            device_id={"dp": s},
            device_id_type=MESH,
        )

    loads["x"].wait()
    loads["norm"].wait()
    x = x_buf[0].astype(F32).reshape(rows, local_d)
    scaled = (x * norm[0:1, :]).astype(BF16)
    squares = square_rows(x)
    for s in range(n_dp):
        for h in range(halves):
            at = s * mine + h * part_rows
            sq_buf[0, h, s, :, pl.ds(0, part_rows)] = squares[0:1, at : at + part_rows]
    loads["w_in"].wait()
    loads["w_gate"].wait()
    parts = jnp.dot(scaled, w_cat[0], preferred_element_type=F32).astype(BF16)
    for s in range(n_dp):
        for h in range(halves):
            at = s * mine + h * part_rows
            part_buf[0, h, s] = parts[at : at + part_rows]
    pl.semaphore_wait(barrier, len(dp_steps) + len(tp_greeted))
    for step in (-hub // 2, hub // 2):
        pl.semaphore_signal(relay, inc=1, device_id={"tp": at_offset(step)}, device_id_type=MESH)
    for h in range(halves):
        for step in reversed(dp_steps):
            send_part(0, h, dp_peer(step))
    for name in later:
        loads[name].wait()
    for layer in range(layers):
        prepare(layer)

    row_lane = lax.broadcasted_iota(jnp.int32, (part_rows, 128), 1)
    row_sub = lax.broadcasted_iota(jnp.int32, (part_rows, 128), 0)

    def mix(layer, h):
        for buf, sem in ((part_recv, part_recv_sem), (sq_recv, sq_recv_sem)):
            others = buf.at[layer, h, pl.ds(0, n_dp - 1)]
            pltpu.make_async_copy(others, others, sem.at[h]).wait()
        total = part_buf[layer, h, i].astype(F32)
        sq = sq_buf[layer, h, i]
        for step in dp_steps:
            s = dp_peer(step)
            total = total + part_recv[layer, h, s].astype(F32)
            sq = sq + sq_recv[layer, h, s]
        mean = jnp.sum(
            jnp.where(row_lane == row_sub, sq[0:1, :], 0.0), axis=1, keepdims=True
        ) / features
        total = total * lax.rsqrt(mean + NORM_EPS)
        u = total[:, :chans].astype(BF16)
        gate = total[:, chans:].astype(BF16).astype(F32)
        u_f = u.astype(F32)
        read = base[layer, h * part_rows : (h + 1) * part_rows] + jnp.dot(
            jnp.concatenate([u, u], axis=1), mix_cat[layer], preferred_element_type=F32
        )
        y = jax.nn.gelu(read + feed[layer : layer + 1, :] * u_f)
        z_buf[layer, h, i] = (y * jax.nn.sigmoid(gate)).astype(BF16)
        for step in reversed(dp_steps):
            z_copy(layer, h, dp_peer(step), i).start()
        return u_f

    def project_streamed(layer, h):
        for step in [(0, 0), *dp_steps]:
            s = dp_peer(step)
            if step != (0, 0):
                z_copy(layer, h, s, s).wait_recv()
            terms = jnp.dot(z_buf[layer, h, s], w_out[layer], preferred_element_type=F32)
            for k in range(per_block):
                owner = s * per_block + k
                term_buf[layer, h, owner] = terms[k * chunk : (k + 1) * chunk].astype(BF16)
            for k in range(per_block):
                owner = s * per_block + k
                o = lax.rem(j - owner + n_tp, n_tp)
                past = lax.div(o, far + 1)
                reach = o + past * (n_tp - 2 * o)
                pl.when((lax.rem(reach, 3) != 0) & (reach != far))(
                    functools.partial(climb, layer, h, owner, o, past, reach)
                )
                pl.when(reach == far)(lambda: up(layer, h, far).start())

    def project_at_once(layer, h):
        await_copies(z_buf.at[layer, h], n_dp - 1, z_recv_sem.at[n_dp])
        z = z_buf[layer, h].reshape(n_dp * part_rows, chans)
        terms = jnp.dot(z, w_out[layer], preferred_element_type=F32)
        term_buf[layer, h] = terms.reshape(n_tp, chunk, local_d).astype(BF16)
        up(layer, h, far).start()
        for o in leaves:
            up(layer, h, o).start()

    def project(layer, h):
        (project_streamed if h == 0 else project_at_once)(layer, h)

    def new_state(layer, h, u_f):
        at = pl.ds(h * part_rows, part_rows)
        spread = jnp.where(own_group[None], u_f[:, None, :], 0.0).astype(BF16)
        spread = spread.reshape(part_rows * groups, chans)
        driven = jnp.dot(spread, drive_high[layer], preferred_element_type=F32) + jnp.dot(
            spread, drive_low[layer], preferred_element_type=F32
        )
        state_out[layer, at] = carried[layer, at] + driven.reshape(part_rows, groups, width)

    def sum_at_hubs(layer, h):
        for group, under in enumerate((far_hub, near_hub)):
            await_copies(term_recv.at[layer, h], len(under), term_recv_sem.at[h, group])
            for o in hubs:
                if children[o][0] not in under:
                    continue
                owner = at_offset(-o)
                total = term_buf[layer, h, owner].astype(F32)
                for c in children[o]:
                    total = total + term_recv[layer, h, c % n_tp].astype(F32)
                if abs(o) == hub:
                    last = term_recv[layer, h, far].astype(F32)
                    total = total + jnp.where(side * o > 0, last, 0.0)
                term_buf[layer, h, owner] = total.astype(BF16)
                up(layer, h, o).start()

    def own_chunk(layer, h):
        total = term_buf[layer, h, j].astype(F32)
        await_copies(term_recv.at[layer, h], len(children[0]), term_recv_sem.at[h, 2])
        for o in sorted(children[0], key=abs):
            total = total + term_recv[layer, h, o % n_tp].astype(F32)
        branch = total.astype(BF16).astype(F32)
        x = of_owner(layer, h, j)[...].astype(F32)
        of_owner(layer + 1, h, j)[...] = (x + branch).astype(BF16)
        for c in sorted(children[0], key=lambda o: -abs(o)):
            down(layer, h, 0, c).start()

    def hand_down(layer, h):
        for o in sorted(hubs, key=abs):
            await_hub_chunk(layer, h, o)
            for c in sorted(children[o], key=lambda c: -abs(c)):
                down(layer, h, o, c).start()
        down(layer, h, hub * side, far * side).start()

    def next_parts(layer, h):
        await_leaf_chunks(layer, h)
        x = x_buf[layer + 1, :, h].astype(F32).reshape(n_dp * part_rows, local_d)
        scaled = (x * norm[layer + 1 : layer + 2, :]).astype(BF16)
        parts = jnp.dot(scaled, w_cat[layer + 1], preferred_element_type=F32)
        part_buf[layer + 1, h] = parts.reshape(n_dp, part_rows, 2 * chans).astype(BF16)
        squares = square_rows(x)
        for s in range(n_dp):
            at = s * part_rows
            sq_buf[layer + 1, h, s, :, pl.ds(0, part_rows)] = squares[0:1, at : at + part_rows]
        for step in reversed(dp_steps):
            send_part(layer + 1, h, dp_peer(step))

    both = range(halves)
    for layer in range(layers):
        u_f = [mix(layer, h) for h in both]
        for h in both:
            project(layer, h)
        for h in both:
            new_state(layer, h, u_f[h])
        if layer == 0:
            pl.semaphore_wait(relay, 2)
        for h in both:
            sum_at_hubs(layer, h)
        for h in both:
            own_chunk(layer, h)
        for h in both:
            hand_down(layer, h)
        if layer + 1 < layers:
            for h in both:
                next_parts(layer, h)
    for h in both:
        await_leaf_chunks(layers - 1, h)
        tokens_out[:, h] = x_buf[layers, :, h]

    await_sends()


def write_out(tokens, state, tokens_out, state_out, sem):
    copies = [
        pltpu.make_async_copy(tokens, tokens_out, sem.at[0]),
        pltpu.make_async_copy(state, state_out, sem.at[1]),
    ]
    for copy in copies:
        copy.start()
    for copy in copies:
        copy.wait()


def on_device(
    n_dp,
    n_tp,
    tokens,
    sequence_lengths,
    recurrent_state,
    norm_weight,
    input_weight,
    gate_weight,
    output_weight,
    negated_real_rate,
    frequency,
    discrete_step,
    group_input_matrix,
    group_output_matrix,
    feedthrough_weight,
    extra_log_decay,
):
    layers, mine, groups, width = recurrent_state.shape
    rows, local_d = tokens.shape
    chans = output_weight.shape[1]
    halves, per_block = 2, n_tp // n_dp
    part_rows = mine // halves
    chunk = part_rows // per_block
    blocked = (n_dp, halves, per_block, chunk, local_d)
    hbm = pl.BlockSpec(memory_space=pltpu.HBM)
    dma = pltpu.SemaphoreType.DMA
    in_hbm = lambda a: pltpu.with_memory_space_constraint(a, pltpu.HBM)
    like = lambda a: pltpu.VMEM(a.shape, a.dtype)
    scratch = [
        pltpu.SMEM(sequence_lengths.shape, sequence_lengths.dtype),
        pltpu.SMEM(discrete_step.shape, discrete_step.dtype),
        pltpu.VMEM((layers + 1, *blocked), BF16),
        like(norm_weight),
        pltpu.VMEM((layers, local_d, 2 * chans), BF16),
        like(output_weight),
        like(extra_log_decay),
        like(recurrent_state),
        like(negated_real_rate),
        like(frequency),
        like(group_input_matrix),
        like(group_output_matrix),
        like(feedthrough_weight),
        dma((16,)),
        pltpu.VMEM((layers, halves, n_dp, part_rows, 2 * chans), BF16),
        pltpu.VMEM((layers, halves, n_dp, part_rows, 2 * chans), BF16),
        dma((1,)),
        dma((halves,)),
        pltpu.VMEM((layers, halves, n_dp, 1, 128), F32),
        pltpu.VMEM((layers, halves, n_dp, 1, 128), F32),
        dma((1,)),
        dma((halves,)),
        pltpu.VMEM((layers, halves, n_dp, part_rows, chans), BF16),
        dma((1,)),
        dma((n_dp + 1,)),
        pltpu.VMEM((layers, halves, n_tp, chunk, local_d), BF16),
        pltpu.VMEM((layers, halves, n_tp, chunk, local_d), BF16),
        dma((1,)),
        dma((halves, 3)),
        dma((1,)),
        dma((halves, 5)),
        pltpu.VMEM((mine, groups, width), F32),
        pltpu.VMEM((layers, mine, groups, width), F32),
        pltpu.VMEM((layers, chans, width), BF16),
        pltpu.VMEM((layers, chans, width), BF16),
        pltpu.VMEM((layers, 2 * chans, chans), BF16),
        pltpu.VMEM((layers, mine, chans), F32),
        pltpu.SemaphoreType.REGULAR,
    ]
    tokens_out, state_out = pl.pallas_call(
        functools.partial(kernel, n_dp, n_tp, n_dp * local_d),
        out_shape=(
            jax.ShapeDtypeStruct(blocked, tokens.dtype),
            jax.ShapeDtypeStruct(recurrent_state.shape, recurrent_state.dtype),
        ),
        in_specs=[hbm] * 14,
        out_specs=(pl.BlockSpec(memory_space=pltpu.VMEM),) * 2,
        scratch_shapes=scratch,
        compiler_params=pltpu.CompilerParams(collective_id=0, has_side_effects=True, vmem_limit_bytes=16 * 2**20),
    )(
        in_hbm(sequence_lengths),
        in_hbm(discrete_step),
        in_hbm(tokens.reshape(blocked)),
        in_hbm(norm_weight),
        in_hbm(input_weight),
        in_hbm(gate_weight),
        in_hbm(extra_log_decay),
        in_hbm(recurrent_state),
        in_hbm(negated_real_rate),
        in_hbm(frequency),
        in_hbm(group_input_matrix),
        in_hbm(group_output_matrix),
        in_hbm(feedthrough_weight),
        in_hbm(output_weight),
    )

    vmem = pl.BlockSpec(memory_space=pltpu.VMEM)
    return pl.pallas_call(
        write_out,
        out_shape=(
            jax.ShapeDtypeStruct(tokens.shape, tokens.dtype),
            jax.ShapeDtypeStruct(recurrent_state.shape, recurrent_state.dtype),
        ),
        in_specs=[vmem, vmem],
        out_specs=(hbm, hbm),
        scratch_shapes=[dma((2,))],
        compiler_params=pltpu.CompilerParams(vmem_limit_bytes=16 * 2**20),
    )(tokens_out.reshape(tokens.shape), state_out)

def solution(mesh):
    in_specs = (
        P("grp", "dp"),
        P(("grp", "dp")),
        P(None, ("grp", "dp"), "tp", None),
        P(None, "dp"),
        P(None, "dp", "tp"),
        P(None, "dp", "tp"),
        P(None, "tp", "dp"),
        P(None, "tp"),
        P(None, "tp"),
        P(None, "tp"),
        P(None, "tp", None, None),
        P(None, "tp", None, None),
        P(None, "tp"),
        P(None, "tp", None),
    )
    out_specs = (P("grp", "dp"), P(None, ("grp", "dp"), "tp", None))
    return jax.shard_map(
        functools.partial(on_device, mesh.shape["dp"], mesh.shape["tp"]),
        mesh=mesh,
        in_specs=in_specs,
        out_specs=out_specs,
        check_vma=False,
    )
```

```python
import functools

import jax
import jax.numpy as jnp
from jax import lax
from jax.experimental import pallas as pl
from jax.experimental.pallas import tpu as pltpu
from jax.sharding import PartitionSpec as P

NORM_EPS = 1e-06
HIGHEST = lax.Precision.HIGHEST
F32 = jnp.float32
BF16 = jnp.bfloat16
MESH = pl.DeviceIdType.MESH


def contract_last(a, b, precision=None):
    return lax.dot_general(
        a, b, (((1,), (1,)), ((), ())), precision=precision, preferred_element_type=F32
    )


def split_two(a):
    high = a.astype(BF16)
    return high, (a - high.astype(F32)).astype(BF16)


def exp_less_one(x, exp_x):
    series = jnp.full_like(x, 1.0 / 3628800.0)
    for factor in (362880.0, 40320.0, 5040.0, 720.0, 120.0, 24.0, 6.0, 2.0, 1.0):
        series = series * x + 1.0 / factor
    return jnp.where(jnp.abs(x) < 0.6, series * x, exp_x - 1.0)


def sign(o):
    return 1 if o > 0 else -1


def step_to_hub(o):
    near = (abs(o) + 1) // 3 * 3
    return abs(o) if near in (0, abs(o)) else abs(o) - near


def kernel(
    n_dp,
    n_tp,
    features,
    lengths_hbm,
    step_hbm,
    tokens_hbm,
    norm_hbm,
    w_in_hbm,
    w_gate_hbm,
    decay_hbm,
    state_hbm,
    rate_hbm,
    freq_hbm,
    b_hbm,
    c_hbm,
    feed_hbm,
    w_out_hbm,
    tokens_out,
    state_out,
    lengths,
    step_width,
    x_buf,
    norm,
    w_cat,
    w_out,
    decay,
    state,
    rate,
    freq,
    b_mat,
    c_mat,
    feed,
    local_sem,
    part_buf,
    part_recv,
    part_send_sem,
    part_recv_sem,
    sq_buf,
    sq_recv,
    sq_send_sem,
    sq_recv_sem,
    z_buf,
    z_send_sem,
    z_recv_sem,
    term_buf,
    term_recv,
    term_send_sem,
    term_recv_sem,
    x_send_sem,
    x_recv_sem,
    pick,
    carried,
    drive_high,
    drive_low,
    mix_cat,
    base,
    relay,
):
    i = lax.axis_index("dp")
    j = lax.axis_index("tp")
    layers, mine, groups, width = state.shape
    half = width // 2
    halves, per_block, chunk, local_d = x_buf.shape[2:]
    rows = n_dp * mine
    part_rows = mine // halves
    chans = w_out.shape[1]
    channel_group = chans // groups

    dp_steps = [(0, 1)] + [
        (d, e) for d in (1, n_dp // 2 - 1, n_dp // 4) for e in (0, 1)
    ]

    def dp_peer(step):
        d, e = step
        return lax.rem(lax.div(i, 2) + d, n_dp // 2) * 2 + lax.rem(lax.rem(i, 2) + e, 2)

    side = 1 - 2 * lax.rem(j, 2)
    far = n_tp // 2
    hub = far - 2
    tree = {o: o - sign(o) * step_to_hub(o) for o in range(1 - far, far) if o}
    children = {p: [o for o in tree if tree[o] == p] for p in [0, *tree]}
    by_reach = sorted(tree, key=lambda o: (-abs(o), o))
    leaves = [o for o in by_reach if not children[o]]
    hubs = [o for o in by_reach if children[o]]

    near_hub = [c for o in hubs if abs(o) != hub for c in children[o]]
    far_hub = [c for o in hubs if abs(o) == hub for c in children[o]] + [far]
    up_group = {o: 0 if o in far_hub else 1 if o in near_hub else 2 for o in [*tree, far]}
    down_group = {o: 1 + hubs.index(o) if o in hubs else 0 for o in [*tree, far]}

    def at_offset(o):
        return lax.rem(j + o + n_tp, n_tp)

    loads = {}
    for n, (name, src, dst) in enumerate(
        [
            ("x", tokens_hbm, x_buf.at[0]),
            ("norm", norm_hbm, norm),
            ("w_in", w_in_hbm.at[0], w_cat.at[0, :, pl.ds(0, chans)]),
            ("w_gate", w_gate_hbm.at[0], w_cat.at[0, :, pl.ds(chans, chans)]),
            ("w_in_1", w_in_hbm.at[1], w_cat.at[1, :, pl.ds(0, chans)]),
            ("w_gate_1", w_gate_hbm.at[1], w_cat.at[1, :, pl.ds(chans, chans)]),
            ("decay", decay_hbm, decay),
            ("state", state_hbm, state),
            ("rate", rate_hbm, rate),
            ("freq", freq_hbm, freq),
            ("b", b_hbm, b_mat),
            ("c", c_hbm, c_mat),
            ("feed", feed_hbm, feed),
            ("lengths", lengths_hbm, lengths),
            ("step", step_hbm, step_width),
            ("w_out", w_out_hbm, w_out),
        ]
    ):
        loads[name] = pltpu.make_async_copy(src, dst, local_sem.at[n])
    for name in ("x", "norm", "w_in", "w_gate"):
        loads[name].start()

    barrier = pltpu.get_barrier_semaphore()
    for step in dp_steps:
        pl.semaphore_signal(barrier, inc=1, device_id={"dp": dp_peer(step)}, device_id_type=MESH)
    tp_greeted = [o for o in (-3, 3, -2, 2, -1, 1)]
    for step in tp_greeted:
        pl.semaphore_signal(barrier, inc=1, device_id={"tp": at_offset(step)}, device_id_type=MESH)

    later = [name for name in loads if name not in ("x", "norm", "w_in", "w_gate")]
    for name in later:
        loads[name].start()

    lane = lax.broadcasted_iota(jnp.int32, (groups, width), 1)
    sub = lax.broadcasted_iota(jnp.int32, (groups, width), 0)
    low = lane < half
    col_group = lax.broadcasted_iota(jnp.int32, (groups, chans), 1) // channel_group
    own_group = col_group == lax.broadcasted_iota(jnp.int32, (groups, chans), 0)
    block_row = lax.broadcasted_iota(jnp.int32, (chans, chans), 0) // channel_group
    block_col = lax.broadcasted_iota(jnp.int32, (chans, chans), 1) // channel_group

    def by_group(ref, layer):
        out = jnp.zeros((groups, width), F32)
        for g in range(groups):
            pair = ref[layer : layer + 1, (g // 2) * width : (g // 2 + 1) * width]
            other = pltpu.roll(pair, half, 1)
            row = jnp.where(low[:1] if g % 2 == 0 else ~low[:1], pair, other)
            out = jnp.where(sub == g, row, out)
        return out

    def prepare(layer):
        dt = jnp.zeros((groups, width), F32)
        for g in range(groups):
            dt = jnp.where(sub == g, step_width[layer, g], dt)
        a_re = by_group(rate, layer)
        a_im = by_group(freq, layer)
        log_mag = -a_re * dt
        turn = a_im * dt
        magnitude = jnp.exp(log_mag)
        cosine = jnp.cos(turn)
        disc_re = magnitude * cosine
        disc_im = magnitude * jnp.sin(turn)
        half_sine = jnp.sin(0.5 * turn)
        numer_re = exp_less_one(log_mag, magnitude) * cosine - 2.0 * half_sine * half_sine
        denom = a_re * a_re + a_im * a_im
        drive_re = (-numer_re * a_re + disc_im * a_im) / denom
        drive_im = (-disc_im * a_re - numer_re * a_im) / denom
        disc_cross = jnp.where(low, -disc_im, disc_im)
        drive_cross = jnp.where(low, -drive_im, drive_im)

        b_l = b_mat[layer]
        drive = drive_re[:, None, :] * b_l + drive_cross[:, None, :] * pltpu.roll(b_l, half, 2)
        drive = drive.reshape(chans, width)
        high, rest = split_two(drive)
        drive_high[layer] = high
        drive_low[layer] = rest
        c_l = jnp.where(low[:1][None], c_mat[layer], -c_mat[layer]).reshape(chans, width)
        mix = jnp.where(block_row == block_col, contract_last(drive, c_l, HIGHEST), 0.0)
        high, rest = split_two(mix)
        mix_cat[layer, :chans] = high
        mix_cat[layer, chans:] = rest

        for r in range(mine):
            offset = lane - (lengths[r] - 1)
            found = jnp.zeros((groups, width), F32)
            for at in range(0, decay.shape[2], width):
                found = jnp.where(offset == -at, decay[layer, :, at : at + width], found)
            pick[r] = found
        extra = jnp.exp(jnp.sum(pick[...], axis=-1, keepdims=True))
        s = state[layer]
        kept = extra * (disc_re[None] * s + disc_cross[None] * pltpu.roll(s, half, 2))
        carried[layer] = kept
        read = contract_last(kept.reshape(mine * groups, width), c_l, HIGHEST)
        read = jnp.where(own_group[None], read.reshape(mine, groups, chans), 0.0)
        base[layer] = jnp.sum(read, axis=1)

    def send_part(layer, h, s):
        for src, dst, ssem, rsem in (
            (part_buf, part_recv, part_send_sem, part_recv_sem),
            (sq_buf, sq_recv, sq_send_sem, sq_recv_sem),
        ):
            pltpu.make_async_remote_copy(
                src_ref=src.at[layer, h, s],
                dst_ref=dst.at[layer, h, i],
                send_sem=ssem.at[0],
                recv_sem=rsem.at[h],
                device_id={"dp": s},
                device_id_type=MESH,
            ).start()

    def await_sends():
        for buf, sem in (
            (part_buf.at[:, :, pl.ds(0, n_dp - 1)], part_send_sem),
            (sq_buf.at[:, :, pl.ds(0, n_dp - 1)], sq_send_sem),
            (z_buf.at[:, :, pl.ds(0, n_dp - 1)], z_send_sem),
            (term_buf.at[:, :, pl.ds(0, n_tp - 1)], term_send_sem),
            (term_buf.at[:, :, pl.ds(0, n_tp - 1)], x_send_sem),
        ):
            pltpu.make_async_copy(buf, buf, sem.at[0]).wait()

    ones = jnp.ones((8, 128), F32)

    def square_rows(x):
        x2 = x * x
        total = x2[:, 0:128]
        for k in range(1, local_d // 128):
            total = total + x2[:, k * 128 : (k + 1) * 128]
        return contract_last(ones, total, HIGHEST)

    def of_owner(layer, h, t):
        return x_buf.at[layer, lax.div(t, per_block), h, lax.rem(t, per_block)]

    def up(layer, h, o):
        hop = 2 * side if o == far else o - tree[o]
        owner = at_offset(-o)
        return pltpu.make_async_remote_copy(
            src_ref=term_buf.at[layer, h, owner],
            dst_ref=term_recv.at[layer, h, o % n_tp],
            send_sem=term_send_sem.at[0],
            recv_sem=term_recv_sem.at[h, up_group[o]],
            device_id={"tp": at_offset(-hop)},
            device_id_type=MESH,
        )

    def climb(layer, h, owner, o, past, reach):
        hop = (1 - 2 * past) * (reach - lax.div(reach + 1, 3) * 3)
        pltpu.make_async_remote_copy(
            src_ref=term_buf.at[layer, h, owner],
            dst_ref=term_recv.at[layer, h, o],
            send_sem=term_send_sem.at[0],
            recv_sem=term_recv_sem.at[h, 2 - lax.div(reach + 1, 3)],
            device_id={"tp": at_offset(-hop)},
            device_id_type=MESH,
        ).start()

    def down(layer, h, o, c):
        piece = of_owner(layer + 1, h, at_offset(-o))
        return pltpu.make_async_remote_copy(
            src_ref=piece,
            dst_ref=piece,
            send_sem=x_send_sem.at[0],
            recv_sem=x_recv_sem.at[h, down_group.get(c if isinstance(c, int) else far, 0)],
            device_id={"tp": at_offset(c - o)},
            device_id_type=MESH,
        )

    def await_copies(buf, count, sem):
        some = buf.at[pl.ds(0, count)]
        pltpu.make_async_copy(some, some, sem).wait()

    def await_hub_chunk(layer, h, o):
        await_copies(term_buf.at[layer, h], 1, x_recv_sem.at[h, down_group[o]])

    def await_leaf_chunks(layer, h):
        await_copies(term_buf.at[layer, h], len(leaves) + 1, x_recv_sem.at[h, 0])

    def z_copy(layer, h, s, owner):
        return pltpu.make_async_remote_copy(
            src_ref=z_buf.at[layer, h, owner],
            dst_ref=z_buf.at[layer, h, owner],
            send_sem=z_send_sem.at[0],
            recv_sem=z_recv_sem.at[owner if h == 0 else n_dp],
            device_id={"dp": s},
            device_id_type=MESH,
        )

    loads["x"].wait()
    loads["norm"].wait()
    x = x_buf[0].astype(F32).reshape(rows, local_d)
    scaled = (x * norm[0:1, :]).astype(BF16)
    squares = square_rows(x)
    for s in range(n_dp):
        for h in range(halves):
            at = s * mine + h * part_rows
            sq_buf[0, h, s, :, pl.ds(0, part_rows)] = squares[0:1, at : at + part_rows]
    loads["w_in"].wait()
    loads["w_gate"].wait()
    parts = jnp.dot(scaled, w_cat[0], preferred_element_type=F32).astype(BF16)
    for s in range(n_dp):
        for h in range(halves):
            at = s * mine + h * part_rows
            part_buf[0, h, s] = parts[at : at + part_rows]
    pl.semaphore_wait(barrier, len(dp_steps) + len(tp_greeted))
    for step in (-hub // 2, hub // 2):
        pl.semaphore_signal(relay, inc=1, device_id={"tp": at_offset(step)}, device_id_type=MESH)
    for h in range(halves):
        for step in reversed(dp_steps):
            send_part(0, h, dp_peer(step))
    for name in later:
        loads[name].wait()
    for layer in range(layers):
        prepare(layer)

    row_lane = lax.broadcasted_iota(jnp.int32, (part_rows, 128), 1)
    row_sub = lax.broadcasted_iota(jnp.int32, (part_rows, 128), 0)

    def mix(layer, h):
        for buf, sem in ((part_recv, part_recv_sem), (sq_recv, sq_recv_sem)):
            others = buf.at[layer, h, pl.ds(0, n_dp - 1)]
            pltpu.make_async_copy(others, others, sem.at[h]).wait()
        total = part_buf[layer, h, i].astype(F32)
        sq = sq_buf[layer, h, i]
        for step in dp_steps:
            s = dp_peer(step)
            total = total + part_recv[layer, h, s].astype(F32)
            sq = sq + sq_recv[layer, h, s]
        mean = jnp.sum(
            jnp.where(row_lane == row_sub, sq[0:1, :], 0.0), axis=1, keepdims=True
        ) / features
        total = total * lax.rsqrt(mean + NORM_EPS)
        u = total[:, :chans].astype(BF16)
        gate = total[:, chans:].astype(BF16).astype(F32)
        u_f = u.astype(F32)
        read = base[layer, h * part_rows : (h + 1) * part_rows] + jnp.dot(
            jnp.concatenate([u, u], axis=1), mix_cat[layer], preferred_element_type=F32
        )
        y = jax.nn.gelu(read + feed[layer : layer + 1, :] * u_f)
        z_buf[layer, h, i] = (y * jax.nn.sigmoid(gate)).astype(BF16)
        for step in reversed(dp_steps):
            z_copy(layer, h, dp_peer(step), i).start()
        return u_f

    def project_streamed(layer, h):
        for step in [(0, 0), *dp_steps]:
            s = dp_peer(step)
            if step != (0, 0):
                z_copy(layer, h, s, s).wait_recv()
            terms = jnp.dot(z_buf[layer, h, s], w_out[layer], preferred_element_type=F32)
            for k in range(per_block):
                owner = s * per_block + k
                term_buf[layer, h, owner] = terms[k * chunk : (k + 1) * chunk].astype(BF16)
            for k in range(per_block):
                owner = s * per_block + k
                o = lax.rem(j - owner + n_tp, n_tp)
                past = lax.div(o, far + 1)
                reach = o + past * (n_tp - 2 * o)
                pl.when((lax.rem(reach, 3) != 0) & (reach != far))(
                    functools.partial(climb, layer, h, owner, o, past, reach)
                )
                pl.when(reach == far)(lambda: up(layer, h, far).start())

    def project_at_once(layer, h):
        await_copies(z_buf.at[layer, h], n_dp - 1, z_recv_sem.at[n_dp])
        z = z_buf[layer, h].reshape(n_dp * part_rows, chans)
        terms = jnp.dot(z, w_out[layer], preferred_element_type=F32)
        term_buf[layer, h] = terms.reshape(n_tp, chunk, local_d).astype(BF16)
        up(layer, h, far).start()
        for o in leaves:
            up(layer, h, o).start()

    def project(layer, h):
        (project_streamed if h == 0 else project_at_once)(layer, h)

    def new_state(layer, h, u_f):
        at = pl.ds(h * part_rows, part_rows)
        spread = jnp.where(own_group[None], u_f[:, None, :], 0.0).astype(BF16)
        spread = spread.reshape(part_rows * groups, chans)
        driven = jnp.dot(spread, drive_high[layer], preferred_element_type=F32) + jnp.dot(
            spread, drive_low[layer], preferred_element_type=F32
        )
        state_out[layer, at] = carried[layer, at] + driven.reshape(part_rows, groups, width)

    def sum_at_hubs(layer, h):
        for group, under in enumerate((far_hub, near_hub)):
            await_copies(term_recv.at[layer, h], len(under), term_recv_sem.at[h, group])
            for o in hubs:
                if children[o][0] not in under:
                    continue
                owner = at_offset(-o)
                total = term_buf[layer, h, owner].astype(F32)
                for c in children[o]:
                    total = total + term_recv[layer, h, c % n_tp].astype(F32)
                if abs(o) == hub:
                    last = term_recv[layer, h, far].astype(F32)
                    total = total + jnp.where(side * o > 0, last, 0.0)
                term_buf[layer, h, owner] = total.astype(BF16)
                up(layer, h, o).start()

    def own_chunk(layer, h):
        total = term_buf[layer, h, j].astype(F32)
        await_copies(term_recv.at[layer, h], len(children[0]), term_recv_sem.at[h, 2])
        for o in sorted(children[0], key=abs):
            total = total + term_recv[layer, h, o % n_tp].astype(F32)
        branch = total.astype(BF16).astype(F32)
        x = of_owner(layer, h, j)[...].astype(F32)
        of_owner(layer + 1, h, j)[...] = (x + branch).astype(BF16)
        for c in sorted(children[0], key=lambda o: -abs(o)):
            down(layer, h, 0, c).start()

    def hand_down(layer, h):
        for o in sorted(hubs, key=abs):
            await_hub_chunk(layer, h, o)
            for c in sorted(children[o], key=lambda c: -abs(c)):
                down(layer, h, o, c).start()
        down(layer, h, hub * side, far * side).start()

    def next_parts(layer, h):
        await_leaf_chunks(layer, h)
        x = x_buf[layer + 1, :, h].astype(F32).reshape(n_dp * part_rows, local_d)
        scaled = (x * norm[layer + 1 : layer + 2, :]).astype(BF16)
        parts = jnp.dot(scaled, w_cat[layer + 1], preferred_element_type=F32)
        part_buf[layer + 1, h] = parts.reshape(n_dp, part_rows, 2 * chans).astype(BF16)
        squares = square_rows(x)
        for s in range(n_dp):
            at = s * part_rows
            sq_buf[layer + 1, h, s, :, pl.ds(0, part_rows)] = squares[0:1, at : at + part_rows]
        for step in reversed(dp_steps):
            send_part(layer + 1, h, dp_peer(step))

    both = range(halves)
    for layer in range(layers):
        u_f = [mix(layer, h) for h in both]
        for h in both:
            project(layer, h)
        if layer == 0:
            pl.semaphore_wait(relay, 2)
        for h in both:
            sum_at_hubs(layer, h)
        for h in both:
            new_state(layer, h, u_f[h])
        for h in both:
            own_chunk(layer, h)
        for h in both:
            hand_down(layer, h)
        if layer + 1 < layers:
            for h in both:
                next_parts(layer, h)
    for h in both:
        await_leaf_chunks(layers - 1, h)
        tokens_out[:, h] = x_buf[layers, :, h]

    await_sends()


def write_out(tokens, state, tokens_out, state_out, sem):
    copies = [
        pltpu.make_async_copy(tokens, tokens_out, sem.at[0]),
        pltpu.make_async_copy(state, state_out, sem.at[1]),
    ]
    for copy in copies:
        copy.start()
    for copy in copies:
        copy.wait()


def on_device(
    n_dp,
    n_tp,
    tokens,
    sequence_lengths,
    recurrent_state,
    norm_weight,
    input_weight,
    gate_weight,
    output_weight,
    negated_real_rate,
    frequency,
    discrete_step,
    group_input_matrix,
    group_output_matrix,
    feedthrough_weight,
    extra_log_decay,
):
    layers, mine, groups, width = recurrent_state.shape
    rows, local_d = tokens.shape
    chans = output_weight.shape[1]
    halves, per_block = 2, n_tp // n_dp
    part_rows = mine // halves
    chunk = part_rows // per_block
    blocked = (n_dp, halves, per_block, chunk, local_d)
    hbm = pl.BlockSpec(memory_space=pltpu.HBM)
    dma = pltpu.SemaphoreType.DMA
    in_hbm = lambda a: pltpu.with_memory_space_constraint(a, pltpu.HBM)
    like = lambda a: pltpu.VMEM(a.shape, a.dtype)
    scratch = [
        pltpu.SMEM(sequence_lengths.shape, sequence_lengths.dtype),
        pltpu.SMEM(discrete_step.shape, discrete_step.dtype),
        pltpu.VMEM((layers + 1, *blocked), BF16),
        like(norm_weight),
        pltpu.VMEM((layers, local_d, 2 * chans), BF16),
        like(output_weight),
        like(extra_log_decay),
        like(recurrent_state),
        like(negated_real_rate),
        like(frequency),
        like(group_input_matrix),
        like(group_output_matrix),
        like(feedthrough_weight),
        dma((16,)),
        pltpu.VMEM((layers, halves, n_dp, part_rows, 2 * chans), BF16),
        pltpu.VMEM((layers, halves, n_dp, part_rows, 2 * chans), BF16),
        dma((1,)),
        dma((halves,)),
        pltpu.VMEM((layers, halves, n_dp, 1, 128), F32),
        pltpu.VMEM((layers, halves, n_dp, 1, 128), F32),
        dma((1,)),
        dma((halves,)),
        pltpu.VMEM((layers, halves, n_dp, part_rows, chans), BF16),
        dma((1,)),
        dma((n_dp + 1,)),
        pltpu.VMEM((layers, halves, n_tp, chunk, local_d), BF16),
        pltpu.VMEM((layers, halves, n_tp, chunk, local_d), BF16),
        dma((1,)),
        dma((halves, 3)),
        dma((1,)),
        dma((halves, 5)),
        pltpu.VMEM((mine, groups, width), F32),
        pltpu.VMEM((layers, mine, groups, width), F32),
        pltpu.VMEM((layers, chans, width), BF16),
        pltpu.VMEM((layers, chans, width), BF16),
        pltpu.VMEM((layers, 2 * chans, chans), BF16),
        pltpu.VMEM((layers, mine, chans), F32),
        pltpu.SemaphoreType.REGULAR,
    ]
    tokens_out, state_out = pl.pallas_call(
        functools.partial(kernel, n_dp, n_tp, n_dp * local_d),
        out_shape=(
            jax.ShapeDtypeStruct(blocked, tokens.dtype),
            jax.ShapeDtypeStruct(recurrent_state.shape, recurrent_state.dtype),
        ),
        in_specs=[hbm] * 14,
        out_specs=(pl.BlockSpec(memory_space=pltpu.VMEM),) * 2,
        scratch_shapes=scratch,
        compiler_params=pltpu.CompilerParams(collective_id=0, has_side_effects=True, vmem_limit_bytes=16 * 2**20),
    )(
        in_hbm(sequence_lengths),
        in_hbm(discrete_step),
        in_hbm(tokens.reshape(blocked)),
        in_hbm(norm_weight),
        in_hbm(input_weight),
        in_hbm(gate_weight),
        in_hbm(extra_log_decay),
        in_hbm(recurrent_state),
        in_hbm(negated_real_rate),
        in_hbm(frequency),
        in_hbm(group_input_matrix),
        in_hbm(group_output_matrix),
        in_hbm(feedthrough_weight),
        in_hbm(output_weight),
    )

    vmem = pl.BlockSpec(memory_space=pltpu.VMEM)
    return pl.pallas_call(
        write_out,
        out_shape=(
            jax.ShapeDtypeStruct(tokens.shape, tokens.dtype),
            jax.ShapeDtypeStruct(recurrent_state.shape, recurrent_state.dtype),
        ),
        in_specs=[vmem, vmem],
        out_specs=(hbm, hbm),
        scratch_shapes=[dma((2,))],
        compiler_params=pltpu.CompilerParams(vmem_limit_bytes=16 * 2**20),
    )(tokens_out.reshape(tokens.shape), state_out)

def solution(mesh):
    in_specs = (
        P("grp", "dp"),
        P(("grp", "dp")),
        P(None, ("grp", "dp"), "tp", None),
        P(None, "dp"),
        P(None, "dp", "tp"),
        P(None, "dp", "tp"),
        P(None, "tp", "dp"),
        P(None, "tp"),
        P(None, "tp"),
        P(None, "tp"),
        P(None, "tp", None, None),
        P(None, "tp", None, None),
        P(None, "tp"),
        P(None, "tp", None),
    )
    out_specs = (P("grp", "dp"), P(None, ("grp", "dp"), "tp", None))
    return jax.shard_map(
        functools.partial(on_device, mesh.shape["dp"], mesh.shape["tp"]),
        mesh=mesh,
        in_specs=in_specs,
        out_specs=out_specs,
        check_vma=False,
    )
```
